512 devices in a mesh: sp: 64 (over z, y), tp: 8 (over x, core).
Axes of the slice: x: 4, y: 8, z: 8, core: 2. Of those that a mesh axis runs over, the one named last changes fastest.
Arguments:
- tokens: bfloat16 [16384, 2048], P('sp', 'tp'), may hold values from -24 to 24
- value_weight: bfloat16 [2, 2048, 2048], P(None, 'sp', 'tp'), may hold values from -0.125 to 0.125
- outer_weight: bfloat16 [2, 2048, 2048], P(None, 'sp', 'tp'), may hold values from -0.125 to 0.125
- inner_weight: bfloat16 [2, 2048, 2048], P(None, 'sp', 'tp'), may hold values from -0.125 to 0.125
- conv_taps: float32 [2, 3, 2048], P(None, None, 'tp'), may hold values from -3.5 to 3.5
- output_weight: bfloat16 [2, 2048, 2048], P(None, 'tp', 'sp'), may hold values from -2 to 2
- norm_gain: float32 [2, 2048], P(None, 'tp'), may hold values from 0.1 to 1.9
- norm_bias: float32 [2, 2048], P(None, 'tp'), may hold values from -3 to 3
Outputs:
- mixed_out: bfloat16 [16384, 2048], P('sp', 'tp')
The draws below stay inside these ranges and needn't reach their ends.
All inputs are finite; a program needn't handle non-finite values.
Results may differ from the reference program's by a relative error of at most 0.03.
Values may be sent and summed in bfloat16 or wider, within the bound.
No kernel may reach another device: no remote copies, remote signals or barrier semaphores. Data moves between devices by JAX's collectives and lax.ppermute only.
A program may use at most 64 MiB of HBM per device.

```python
import jax
import jax.numpy as jnp
from jax import lax

D = 2048
CW = 2048
CONV_K = 3
LAYERS = 2
TOKENS = 16384
N_TP = 8


def column_scale(key, width):
    position = jnp.arange(width, dtype=jnp.float32) / width
    rough = jax.random.uniform(key, (width,), jnp.float32, 0.6, 1.4)
    return jnp.exp(jnp.log(4.0) * position) * rough


def draw_tokens(key, part):
    first, second = jax.random.split(jax.random.fold_in(key, 11), 2)
    scales = column_scale(second, D)
    base = jnp.clip(jax.random.normal(first, (TOKENS, D), jnp.float32), -5.0, 5.0)
    return jnp.clip(base * scales[None, :], -24.0, 24.0).astype(jnp.bfloat16)


def draw_output_weight(key, part):
    first, second = jax.random.split(jax.random.fold_in(key, 23), 2)
    scales = column_scale(second, D)
    base = jnp.clip(jax.random.normal(first, (LAYERS, CW, D), jnp.float32), -5.0, 5.0)
    values = base * scales[None, None, :] * CW ** (-0.5)
    return jnp.clip(values, -2.0, 2.0).astype(jnp.bfloat16)


def block_levels(rng, shape, pieces, low, top_value):
    loudness, own = 1.0, jax.random.fold_in(rng, 6)
    for dim, shards_of in pieces:
        draws = jnp.exp(jax.random.uniform(jax.random.fold_in(own, dim), (shards_of,), jnp.float32, low / len(pieces), top_value / len(pieces)))
        loudness = loudness * jnp.repeat(draws, shape[dim] // shards_of).reshape([-1 if axis == dim else 1 for axis in range(len(shape))])
    return loudness


def scatter_about(own_key, extent, spread, reach, cuts=(), kind=jnp.bfloat16):
    level = block_levels(own_key, extent, cuts, -0.22, 0.18) if cuts else 1.0
    array = jax.random.normal(own_key, extent, jnp.float32) * spread * level
    return jnp.minimum(jnp.maximum(array, -reach), reach).astype(kind)


def setup_inputs(seed: int = 0) -> dict:
    key_list = jax.random.split(jax.random.key(seed), 9)
    return {
        "tokens": draw_tokens(jax.random.fold_in(key_list[8], 71), 0),
        "value_weight": scatter_about(key_list[1], (LAYERS, D, CW), D ** -0.5, 0.125, ((1, 64), (2, 8))),
        "outer_weight": scatter_about(key_list[2], (LAYERS, D, CW), D ** -0.5, 0.125, ((1, 64), (2, 8))),
        "inner_weight": scatter_about(key_list[3], (LAYERS, D, CW), D ** -0.5, 0.125, ((1, 64), (2, 8))),
        "conv_taps": scatter_about(key_list[4], (LAYERS, CONV_K, CW), CONV_K ** -0.5, 3.5, ((2, 8),), jnp.float32),
        "output_weight": draw_output_weight(jax.random.fold_in(key_list[8], 71), 0),
        "norm_gain": jnp.clip(1.0 + 0.18 * jax.random.normal(key_list[6], (LAYERS, D), jnp.float32), 0.1, 1.9),
        "norm_bias": scatter_about(key_list[7], (LAYERS, D), 0.5, 3.0, ((1, 8),), jnp.float32),
    }


def reference(tokens, value_weight, outer_weight, inner_weight, conv_taps, output_weight, norm_gain, norm_bias):
    alpha = (2.0 * LAYERS) ** 0.25
    state = tokens
    width = CW // N_TP
    for layer in range(LAYERS):
        u_part = jnp.dot(state, value_weight[layer], preferred_element_type=jnp.float32).astype(jnp.bfloat16)
        outer = jnp.dot(state, outer_weight[layer], preferred_element_type=jnp.float32).astype(jnp.bfloat16)
        inner = jnp.dot(state, inner_weight[layer], preferred_element_type=jnp.float32).astype(jnp.bfloat16)
        gated_in = inner.astype(jnp.float32) * u_part.astype(jnp.float32)
        padded = jnp.concatenate([jnp.zeros((CONV_K - 1, CW), jnp.float32), gated_in], axis=0)
        conv = jnp.zeros_like(gated_in)
        for tap in range(CONV_K):
            conv = conv + conv_taps[layer, tap][None, :] * padded[tap:tap + gated_in.shape[0]]
        gated = (outer.astype(jnp.float32) * conv).astype(jnp.bfloat16)
        branch = jnp.zeros((gated.shape[0], D), jnp.float32)
        for block in range(N_TP):
            part_sum = jnp.dot(gated[:, block * width:(block + 1) * width], output_weight[layer, block * width:(block + 1) * width], preferred_element_type=jnp.float32).astype(jnp.bfloat16)
            branch = branch + lax.optimization_barrier(part_sum).astype(jnp.float32)
        pre = alpha * state.astype(jnp.float32) + branch
        mean = lax.optimization_barrier(jnp.mean(pre, axis=-1, keepdims=True))
        var = lax.optimization_barrier(jnp.mean(jnp.square(pre - mean), axis=-1, keepdims=True))
        normed = (pre - mean) * lax.rsqrt(var + 1e-05)
        state = (normed * norm_gain[layer][None, :] + norm_bias[layer][None, :]).astype(jnp.bfloat16)
    return state
```

```python
import jax
import jax.numpy as jnp
from jax import lax
from jax.sharding import Mesh, PartitionSpec as P

D = 2048
LAYERS = 2
TP = ("x", "core")
SP = ("z", "y")
HALO = 16
IN_UP, OUT_UP = 2.0**18, 2.0**14


def bf(x):
    return x.astype(jnp.bfloat16)


def f32(x):
    return x.astype(jnp.float32)


def rounded(x):
    return lax.reduce_precision(x, exponent_bits=8, mantissa_bits=7)


def thirds(x):
    a = rounded(x)
    b = rounded(x - a)
    c = rounded(x - a - b)
    return jnp.stack([bf(a), bf(b), bf(c)])


def packed(value, outer, inner, out, layer):
    return jnp.concatenate([value[layer], outer[layer], inner[layer], out[layer].T], axis=1)


def norm(pre, gain, bias):
    mean = jnp.mean(pre, axis=-1, keepdims=True)
    cent = pre - mean
    var = jnp.mean(cent * cent, axis=-1, keepdims=True)
    return bf(cent * lax.rsqrt(var + 1e-05) * gain + bias)


def gated_rows(x, w_in, down, taps, first, head):
    width = w_in.shape[1] // 3
    acc = jnp.dot(x, w_in, preferred_element_type=jnp.float32) * down
    u, outer, inner = (f32(bf(acc[:, i * width : (i + 1) * width])) for i in range(3))
    z = inner * u
    row = lax.broadcasted_iota(jnp.int32, z.shape, 0)
    z = jnp.where(jnp.logical_and(first, row < head), 0.0, z)
    conv = taps[2] * z[2:] + taps[1] * z[1:-1] + taps[0] * z[:-2]
    return bf(outer[2:] * conv)


def out_product(g, w_out_t, down):
    return lax.dot_general(g, w_out_t, (((1,), (1,)), ((), ())), preferred_element_type=jnp.float32) * down


def pair_sum(main, extra, w_out_t, down, core):
    blocks = main.reshape(4, 2, 32, -1)
    mine = jnp.where(core == 0, blocks[:, 0], blocks[:, 1]).reshape(128, -1)
    other = jnp.where(core == 0, blocks[:, 1], blocks[:, 0]).reshape(128, -1)
    if extra is not None:
        mine = jnp.concatenate([mine, extra], axis=0)
        other = jnp.concatenate([other, extra], axis=0)
    sent = bf(out_product(other, w_out_t, down))
    got = lax.ppermute(sent, "core", [(0, 1), (1, 0)])
    return out_product(mine, w_out_t, down) + f32(got)


def shards(tokens, value, outer, inner, taps, out, gain, bias):
    alpha = (2.0 * LAYERS) ** 0.25
    core = lax.axis_index("core")
    sp = lax.axis_index(SP)
    tp = lax.axis_index(TP)
    first = sp == 0
    late = lax.all_gather(packed(value, outer, inner, out, 1), SP, axis=0, tiled=True)

    halo = lax.ppermute(tokens[-HALO:], SP, [(i, i + 1) for i in range(63)])
    params = jnp.concatenate([gain, bias], axis=0)
    parts = thirds(params).reshape(12, 256)
    parts = jnp.concatenate([parts, jnp.zeros((4, 256), jnp.bfloat16)], axis=0)
    mine = jnp.concatenate([halo, tokens, parts], axis=0)
    everyone = lax.all_to_all(jnp.broadcast_to(mine[None], (8, *mine.shape)), TP, 0, 0, tiled=True)

    scale = jnp.where(jnp.arange(1024) < 768, IN_UP, OUT_UP)
    early = (f32(packed(value, outer, inner, out, 0)) * scale).astype(jnp.float16)
    early = lax.all_gather(early, SP, axis=0, tiled=True)
    early = bf(early)

    whole = jnp.moveaxis(everyone, 0, 1).reshape(288, D)
    table = f32(whole[272:284]).reshape(3, 4, D)
    table = table[0] + table[1] + table[2]
    x0 = whole[:272]

    g = gated_rows(x0, early[:, :768], 1.0 / IN_UP, taps[0], first, HALO)
    branch = pair_sum(g[HALO - 2 :], g[HALO - 10 : HALO - 2], early[:, 768:], 1.0 / OUT_UP, core)
    main = bf(branch[:128]).reshape(4, 32, D)
    extra = bf(branch[134:136]).reshape(32, 128)
    send = jnp.concatenate([main, jnp.broadcast_to(extra[None], (4, 32, 128))], axis=2)
    got = jnp.sum(f32(lax.all_to_all(send, "x", 0, 0, tiled=True)), axis=0)
    own = lax.dynamic_slice_in_dim(x0, HALO + 32 * tp, 32, axis=0)
    pre = jnp.concatenate([alpha * f32(own) + got[:, :D], alpha * f32(x0[HALO - 2 : HALO]) + got[:, D:].reshape(2, D)], axis=0)
    state = norm(pre, table[0], table[2])
    own = state[:32]
    every = lax.all_gather(own.astype(jnp.float16), TP, axis=0, tiled=True)
    x1 = jnp.concatenate([jnp.zeros((6, D), jnp.bfloat16), state[32:], bf(every)], axis=0)

    g = gated_rows(x1, late[:, :768], 1.0, taps[1], first, 8)
    branch = pair_sum(g[6:], None, late[:, 768:], 1.0, core)
    got = lax.all_to_all(bf(branch).reshape(4, 32, D), "x", 0, 0, tiled=True)
    pre = alpha * f32(own) + jnp.sum(f32(got), axis=0)
    state = norm(pre, table[1], table[3])
    back = jnp.moveaxis(state.reshape(32, 8, 256), 1, 0)
    return lax.all_to_all(back, TP, 0, 0, tiled=True).reshape(256, 256)


def solution(mesh):
    mesh = Mesh(mesh.devices.reshape(8, 8, 4, 2), ("z", "y", "x", "core"))
    in_specs = (
        P(SP, TP),
        P(None, SP, TP),
        P(None, SP, TP),
        P(None, SP, TP),
        P(None, None, TP),
        P(None, TP, SP),
        P(None, TP),
        P(None, TP),
    )
    return jax.shard_map(shards, mesh=mesh, in_specs=in_specs, out_specs=P(SP, TP), check_vma=False)
```

```python
import jax
import jax.numpy as jnp
from jax import lax
from jax.experimental import pallas as pl
from jax.experimental.pallas import tpu as pltpu
from jax.sharding import Mesh, PartitionSpec as P


D = 2048
LAYERS = 2
TP = ("x", "core")
SP = ("z", "y")
HALO = 16
IN_UP, OUT_UP = 2.0**18, 2.0**14


def bf(x):
    return x.astype(jnp.bfloat16)


def f32(x):
    return x.astype(jnp.float32)


def fetch(sources, targets, sems):
    copies = [pltpu.make_async_copy(a, b, sems.at[i]) for i, (a, b) in enumerate(zip(sources, targets))]
    for copy in copies:
        copy.start()
    for copy in copies:
        copy.wait()


HBM = pl.BlockSpec(memory_space=pltpu.HBM)
VMEM = pl.BlockSpec(memory_space=pltpu.VMEM)


def pack_kernel(value, outer, inner, out_t, early, late, held, sems):
    fetch((value, outer, inner, out_t), [held.at[i] for i in range(4)], sems)
    for i in range(4):
        at = slice(256 * i, 256 * (i + 1))
        early[:, at] = bf(f32(held[i, 0]) * (IN_UP if i < 3 else OUT_UP))
        late[:, at] = held[i, 1]


def pack(value, outer, inner, out_t):
    shape = jax.ShapeDtypeStruct((32, 1024), jnp.bfloat16)
    return pl.pallas_call(
        pack_kernel,
        in_specs=[HBM] * 4,
        out_specs=(VMEM, VMEM),
        out_shape=(shape, shape),
        scratch_shapes=[pltpu.VMEM((4, 2, 32, 256), jnp.bfloat16), pltpu.SemaphoreType.DMA((4,))],
        cost_estimate=pl.CostEstimate(flops=2000000, bytes_accessed=262144, transcendentals=0),
    )(value, outer, inner, out_t)


def stack_kernel(halo, tokens, gain, bias, copies, held, left, sems):
    fetch((tokens, gain, bias), (held.at[HALO : HALO + 256], left.at[0:2], left.at[2:4]), sems)
    held[:HALO] = halo[...]
    rest = left[...]
    terms = []
    for _ in range(3):
        terms.append(f32(bf(rest)))
        rest = rest - terms[-1]
    terms.append(jnp.zeros_like(rest))
    held[HALO + 256 :] = bf(jnp.concatenate(terms, axis=0))
    fetch([held] * 8, [copies.at[i] for i in range(8)], sems)


def stacked_copies(halo, tokens, gain, bias):
    return pl.pallas_call(
        stack_kernel,
        in_specs=[VMEM, HBM, HBM, HBM],
        out_specs=HBM,
        out_shape=jax.ShapeDtypeStruct((8, 288, 256), jnp.bfloat16),
        scratch_shapes=[
            pltpu.VMEM((288, 256), jnp.bfloat16),
            pltpu.VMEM((4, 256), jnp.float32),
            pltpu.SemaphoreType.DMA((8,)),
        ],
        cost_estimate=pl.CostEstimate(flops=2000000, bytes_accessed=1400000, transcendentals=0),
    )(halo, tokens, gain, bias)


def norm(pre, gain, bias):
    mean = jnp.mean(pre, axis=-1, keepdims=True)
    cent = pre - mean
    var = jnp.mean(cent * cent, axis=-1, keepdims=True)
    return bf(cent * lax.rsqrt(var + 1e-05) * gain + bias)


def shards(tokens, value, outer, inner, taps, out, gain, bias):
    taps = jnp.swapaxes(taps, 0, 1)
    halo = lax.ppermute(tokens[-HALO:], SP, [(i, i + 1) for i in range(63)])
    early, late = pack(value, outer, inner, jnp.swapaxes(out, 1, 2))
    late = lax.all_gather(late, SP, axis=0, tiled=True)
    copies = stacked_copies(halo, tokens, gain, bias)
    everyone = lax.all_to_all(copies, TP, 0, 0, tiled=True)
    early = lax.all_gather(early.astype(jnp.float16), SP, axis=0, tiled=True)

    early, everyone = lax.optimization_barrier((early, everyone))
    sent, mine, kept, table = front(everyone, [bf(early[:, 256 * i : 256 * (i + 1)]) for i in range(4)], taps)
    got = lax.ppermute(sent, "core", [(0, 1), (1, 0)])
    got = lax.all_to_all(folded(got, mine), "x", 0, 0, tiled=True)
    own, before = middle(got, kept, table)
    every = lax.all_gather(own.astype(jnp.float16), TP, axis=0, tiled=True)

    sent, mine = rear(bf(every), before, late, taps)
    got = lax.ppermute(sent, "core", [(0, 1), (1, 0)])
    got = lax.all_to_all(bf(f32(got) + mine).reshape(4, 32, D), "x", 0, 0, tiled=True)
    return lax.all_to_all(last(got, own, table), TP, 0, 0, tiled=True).reshape(256, 256)


def front_kernel(xs, w_u, w_outer, w_inner, w_out, taps, sent, mine, kept, table, x, g, half):
    core = lax.axis_index("core")
    tp = 2 * lax.axis_index("x") + core
    first = jnp.logical_and(lax.axis_index("z") == 0, lax.axis_index("y") == 0)
    rows = HALO + 256
    for j in range(8):
        x[:, 256 * j : 256 * (j + 1)] = xs[j, :rows]
        tail = f32(xs[j, rows:])
        table[:, 256 * j : 256 * (j + 1)] = tail[0:4] + tail[4:8] + tail[8:12]
    u, outer, inner = (
        f32(bf(jnp.dot(x[...], w[...], preferred_element_type=jnp.float32) * (1.0 / IN_UP)))
        for w in (w_u, w_outer, w_inner)
    )
    row = lax.broadcasted_iota(jnp.int32, u.shape, 0)
    z = jnp.where(jnp.logical_and(first, row < HALO), 0.0, inner * u)
    conv = taps[2, 0:1] * z + taps[1, 0:1] * pltpu.roll(z, 1, 0) + taps[0, 0:1] * pltpu.roll(z, 2, 0)
    g[...] = bf(outer * conv)
    alpha = (2.0 * LAYERS) ** 0.25
    kept[:32] = alpha * f32(x[pl.ds(pl.multiple_of(HALO + 32 * tp, 16), 32)])
    kept[32:] = alpha * f32(x[HALO - 8 : HALO])
    half[128:] = g[HALO - 8 : HALO]
    for target, which in ((sent, 1 - core), (mine, core)):
        for i in range(4):
            half[32 * i : 32 * (i + 1)] = g[pl.ds(pl.multiple_of(HALO + 64 * i + 32 * which, 16), 32)]
        for n in range(4):
            at = slice(512 * n, 512 * (n + 1))
            part = lax.dot_general(
                half[...], w_out[at], (((1,), (1,)), ((), ())), preferred_element_type=jnp.float32
            ) * (1.0 / OUT_UP)
            target[:, at] = part.astype(target.dtype)


def front(xs, weights, taps):
    shape = jax.ShapeDtypeStruct
    return pl.pallas_call(
        front_kernel,
        out_shape=(
            shape((136, D), jnp.bfloat16),
            shape((136, D), jnp.float32),
            shape((40, D), jnp.float32),
            shape((4, D), jnp.float32),
        ),
        scratch_shapes=[
            pltpu.VMEM((HALO + 256, D), jnp.bfloat16),
            pltpu.VMEM((HALO + 256, 256), jnp.bfloat16),
            pltpu.VMEM((136, 256), jnp.bfloat16),
        ],
        compiler_params=pltpu.CompilerParams(vmem_limit_bytes=20 * 2**20),
        cost_estimate=pl.CostEstimate(flops=1200000000, bytes_accessed=7000000, transcendentals=0),
    )(xs, *weights, taps)


def fold_kernel(got, mine, out, strip):
    total = f32(got[...]) + mine[...]
    for i in range(4):
        out[i, :, :D] = bf(total[32 * i : 32 * (i + 1)])
    for t in range(2):
        for r in range(16):
            strip[16 * t + r : 16 * t + r + 1] = total[134 + t : 135 + t, 128 * r : 128 * (r + 1)]
    for i in range(4):
        out[i, :, D:] = bf(strip[...])


def folded(got, mine):
    return pl.pallas_call(
        fold_kernel,
        out_shape=jax.ShapeDtypeStruct((4, 32, D + 128), jnp.bfloat16),
        scratch_shapes=[pltpu.VMEM((32, 128), jnp.float32)],
        compiler_params=pltpu.CompilerParams(vmem_limit_bytes=6 * 2**20),
        cost_estimate=pl.CostEstimate(flops=1000000, bytes_accessed=2200000, transcendentals=0),
    )(got, mine)


def middle_kernel(got, kept, table, own, before, wide):
    total = f32(got[0]) + f32(got[1]) + f32(got[2]) + f32(got[3])
    wide[...] = jnp.zeros_like(wide)
    for t in range(2):
        for r in range(16):
            wide[6 + t : 7 + t, 128 * r : 128 * (r + 1)] = total[16 * t + r : 16 * t + r + 1, D:]
    gain, bias = table[0:1], table[2:3]
    own[...] = norm(kept[:32] + total[:, :D], gain, bias)
    before[...] = norm(kept[32:] + wide[...], gain, bias)


def middle(got, kept, table):
    shape = jax.ShapeDtypeStruct
    return pl.pallas_call(
        middle_kernel,
        out_shape=(shape((32, D), jnp.bfloat16), shape((8, D), jnp.bfloat16)),
        scratch_shapes=[pltpu.VMEM((8, D), jnp.float32)],
        compiler_params=pltpu.CompilerParams(vmem_limit_bytes=6 * 2**20),
        cost_estimate=pl.CostEstimate(flops=2000000, bytes_accessed=1200000, transcendentals=100),
    )(got, kept, table)


def rear_kernel(x, before, w, taps, sent, mine, held, acc, g, half, sems):
    core = lax.axis_index("core")
    first = jnp.logical_and(lax.axis_index("z") == 0, lax.axis_index("y") == 0)
    step = D // 4
    copies = [
        pltpu.make_async_copy(w.at[step * i : step * (i + 1)], held.at[step * i : step * (i + 1)], sems.at[i])
        for i in range(4)
    ]
    for copy in copies:
        copy.start()
    for i, copy in enumerate(copies):
        copy.wait()
        at = slice(step * i, step * (i + 1))
        for rows, source in ((slice(0, 8), before), (slice(8, 264), x)):
            part = jnp.dot(source[:, at], held[at, :768], preferred_element_type=jnp.float32)
            acc[rows] = part if i == 0 else acc[rows] + part
    u, outer, inner = (f32(bf(acc[:, 256 * i : 256 * (i + 1)])) for i in range(3))
    row = lax.broadcasted_iota(jnp.int32, u.shape, 0)
    z = jnp.where(jnp.logical_and(first, row < 8), 0.0, inner * u)
    conv = taps[2, 1:2] * z + taps[1, 1:2] * pltpu.roll(z, 1, 0) + taps[0, 1:2] * pltpu.roll(z, 2, 0)
    g[...] = bf((outer * conv)[8:])
    for target, which in ((sent, 1 - core), (mine, core)):
        for i in range(4):
            half[32 * i : 32 * (i + 1)] = g[pl.ds(pl.multiple_of(64 * i + 32 * which, 16), 32)]
        for n in range(4):
            at = slice(512 * n, 512 * (n + 1))
            part = lax.dot_general(
                half[...], held[at, 768:], (((1,), (1,)), ((), ())), preferred_element_type=jnp.float32
            )
            target[:, at] = part.astype(target.dtype)


def rear(x, before, w, taps):
    shape = jax.ShapeDtypeStruct
    return pl.pallas_call(
        rear_kernel,
        in_specs=[VMEM, VMEM, HBM, VMEM],
        out_specs=(VMEM, VMEM),
        out_shape=(shape((128, D), jnp.bfloat16), shape((128, D), jnp.float32)),
        scratch_shapes=[
            pltpu.VMEM((D, 1024), jnp.bfloat16),
            pltpu.VMEM((264, 768), jnp.float32),
            pltpu.VMEM((256, 256), jnp.bfloat16),
            pltpu.VMEM((128, 256), jnp.bfloat16),
            pltpu.SemaphoreType.DMA((4,)),
        ],
        compiler_params=pltpu.CompilerParams(vmem_limit_bytes=50 * 2**20),
        cost_estimate=pl.CostEstimate(flops=1200000000, bytes_accessed=7000000, transcendentals=0),
    )(x, before, w, taps)


def last_kernel(got, own, table, out):
    total = f32(got[0]) + f32(got[1]) + f32(got[2]) + f32(got[3])
    alpha = (2.0 * LAYERS) ** 0.25
    state = norm(alpha * f32(own[...]) + total, table[1:2], table[3:4])
    for i in range(8):
        out[i] = state[:, 256 * i : 256 * (i + 1)]


def last(got, own, table):
    return pl.pallas_call(
        last_kernel,
        out_shape=jax.ShapeDtypeStruct((8, 32, 256), jnp.bfloat16),
        compiler_params=pltpu.CompilerParams(vmem_limit_bytes=6 * 2**20),
        cost_estimate=pl.CostEstimate(flops=2000000, bytes_accessed=1200000, transcendentals=100),
    )(got, own, table)


def solution(mesh):
    mesh = Mesh(mesh.devices.reshape(8, 8, 4, 2), ("z", "y", "x", "core"))
    in_specs = (
        P(SP, TP),
        P(None, SP, TP),
        P(None, SP, TP),
        P(None, SP, TP),
        P(None, None, TP),
        P(None, TP, SP),
        P(None, TP),
        P(None, TP),
    )
    return jax.shard_map(shards, mesh=mesh, in_specs=in_specs, out_specs=P(SP, TP), check_vma=False)
```

```python
import jax
import jax.numpy as jnp
from jax import lax
from jax.experimental import pallas as pl
from jax.experimental.pallas import tpu as pltpu
from jax.sharding import Mesh, PartitionSpec as P


D = 2048
LAYERS = 2
TP = ("x", "core")
SP = ("z", "y")
HALO = 16
IN_UP, OUT_UP = 2.0**18, 2.0**14


def bf(x):
    return x.astype(jnp.bfloat16)


def f32(x):
    return x.astype(jnp.float32)


def fetch(sources, targets, sems):
    copies = [pltpu.make_async_copy(a, b, sems.at[i]) for i, (a, b) in enumerate(zip(sources, targets))]
    for copy in copies:
        copy.start()
    for copy in copies:
        copy.wait()


HBM = pl.BlockSpec(memory_space=pltpu.HBM)
VMEM = pl.BlockSpec(memory_space=pltpu.VMEM)


def pack_kernel(value, outer, inner, out_t, early, late, held, sems):
    fetch((value, outer, inner, out_t), [held.at[i] for i in range(4)], sems)
    for i in range(4):
        at = slice(256 * i, 256 * (i + 1))
        early[:, at] = bf(f32(held[i, 0]) * (IN_UP if i < 3 else OUT_UP))
        late[:, at] = held[i, 1]


def pack(value, outer, inner, out_t):
    shape = jax.ShapeDtypeStruct((32, 1024), jnp.bfloat16)
    return pl.pallas_call(
        pack_kernel,
        in_specs=[HBM] * 4,
        out_specs=(VMEM, VMEM),
        out_shape=(shape, shape),
        scratch_shapes=[pltpu.VMEM((4, 2, 32, 256), jnp.bfloat16), pltpu.SemaphoreType.DMA((4,))],
        cost_estimate=pl.CostEstimate(flops=2000000, bytes_accessed=262144, transcendentals=0),
    )(value, outer, inner, out_t)


def stack_kernel(halo, tokens, gain, bias, copies, held, left, sems):
    fetch((tokens, gain, bias), (held.at[HALO : HALO + 256], left.at[0:2], left.at[2:4]), sems)
    held[:HALO] = halo[...]
    rest = left[...]
    terms = []
    for _ in range(3):
        terms.append(f32(bf(rest)))
        rest = rest - terms[-1]
    terms.append(jnp.zeros_like(rest))
    held[HALO + 256 :] = bf(jnp.concatenate(terms, axis=0))
    fetch([held] * 8, [copies.at[i] for i in range(8)], sems)


def stacked_copies(halo, tokens, gain, bias):
    return pl.pallas_call(
        stack_kernel,
        in_specs=[VMEM, HBM, HBM, HBM],
        out_specs=HBM,
        out_shape=jax.ShapeDtypeStruct((8, 288, 256), jnp.bfloat16),
        scratch_shapes=[
            pltpu.VMEM((288, 256), jnp.bfloat16),
            pltpu.VMEM((4, 256), jnp.float32),
            pltpu.SemaphoreType.DMA((8,)),
        ],
        cost_estimate=pl.CostEstimate(flops=2000000, bytes_accessed=1400000, transcendentals=0),
    )(halo, tokens, gain, bias)


def norm(pre, gain, bias):
    mean = jnp.mean(pre, axis=-1, keepdims=True)
    cent = pre - mean
    var = jnp.mean(cent * cent, axis=-1, keepdims=True)
    return bf(cent * lax.rsqrt(var + 1e-05) * gain + bias)


def shards(tokens, value, outer, inner, taps, out, gain, bias):
    taps = jnp.swapaxes(taps, 0, 1)
    halo = lax.ppermute(tokens[-HALO:], SP, [(i, i + 1) for i in range(63)])
    early, late = pack(value, outer, inner, jnp.swapaxes(out, 1, 2))
    late = lax.all_gather(late, SP, axis=0, tiled=True)
    copies = stacked_copies(halo, tokens, gain, bias)
    everyone = lax.all_to_all(copies, TP, 0, 0, tiled=True)
    early = lax.all_gather(early.astype(jnp.float16), SP, axis=0, tiled=True)

    sent, mine, kept, table = front(everyone, [bf(early[:, 256 * i : 256 * (i + 1)]) for i in range(4)], taps)
    got = lax.ppermute(sent, "core", [(0, 1), (1, 0)])
    got = lax.all_to_all(folded(got, mine), "x", 0, 0, tiled=True)
    own, before = middle(got, kept, table)
    every = lax.all_gather(own.astype(jnp.float16), TP, axis=0, tiled=True)

    sent, mine = rear(bf(every), before, late, taps)
    got = lax.ppermute(sent, "core", [(0, 1), (1, 0)])
    got = lax.all_to_all(bf(f32(got) + f32(mine)).reshape(4, 32, D), "x", 0, 0, tiled=True)
    return lax.all_to_all(last(got, own, table), TP, 0, 0, tiled=True).reshape(256, 256)


def front_kernel(xs, w_u, w_outer, w_inner, w_out, taps, sent, mine, kept, table, x, tails, g, half, held, sems):
    core = lax.axis_index("core")
    tp = 2 * lax.axis_index("x") + core
    first = jnp.logical_and(lax.axis_index("z") == 0, lax.axis_index("y") == 0)
    rows = HALO + 256
    copies = [pltpu.make_async_copy(w, held.at[i], sems.at[i]) for i, w in enumerate((w_u, w_outer, w_inner, w_out))]
    for j in range(8):
        at = slice(256 * j, 256 * (j + 1))
        copies.append(pltpu.make_async_copy(xs.at[j, 0:rows], x.at[:, at], sems.at[4 + j]))
        copies.append(pltpu.make_async_copy(xs.at[j, rows : rows + 16], tails.at[:, at], sems.at[12 + j]))
    for copy in copies[4:] + copies[:4]:
        copy.start()
    for copy in copies[4:]:
        copy.wait()
    tail = f32(tails[...])
    table[...] = tail[0:4] + tail[4:8] + tail[8:12]
    alpha = (2.0 * LAYERS) ** 0.25
    kept[:32] = alpha * f32(x[pl.ds(pl.multiple_of(HALO + 32 * tp, 16), 32)])
    kept[32:] = alpha * f32(x[HALO - 8 : HALO])
    products = []
    for i in range(3):
        copies[i].wait()
        part = jnp.dot(x[...], held[i], preferred_element_type=jnp.float32)
        products.append(f32(bf(part * (1.0 / IN_UP))))
    u, outer, inner = products
    row = lax.broadcasted_iota(jnp.int32, u.shape, 0)
    z = jnp.where(jnp.logical_and(first, row < HALO), 0.0, inner * u)
    conv = taps[2, 0:1] * z + taps[1, 0:1] * pltpu.roll(z, 1, 0) + taps[0, 0:1] * pltpu.roll(z, 2, 0)
    g[...] = bf(outer * conv)
    half[128:] = g[HALO - 8 : HALO]
    copies[3].wait()
    for target, which in ((sent, 1 - core), (mine, core)):
        for i in range(4):
            half[32 * i : 32 * (i + 1)] = g[pl.ds(pl.multiple_of(HALO + 64 * i + 32 * which, 16), 32)]
        for n in range(4):
            at = slice(512 * n, 512 * (n + 1))
            part = lax.dot_general(
                half[...], held[3, at], (((1,), (1,)), ((), ())), preferred_element_type=jnp.float32
            ) * (1.0 / OUT_UP)
            target[:, at] = part.astype(target.dtype)


def front(xs, weights, taps):
    shape = jax.ShapeDtypeStruct
    return pl.pallas_call(
        front_kernel,
        in_specs=[HBM, HBM, HBM, HBM, HBM, VMEM],
        out_specs=(VMEM,) * 4,
        out_shape=(
            shape((136, D), jnp.bfloat16),
            shape((136, D), jnp.bfloat16),
            shape((40, D), jnp.float32),
            shape((4, D), jnp.float32),
        ),
        scratch_shapes=[
            pltpu.VMEM((HALO + 256, D), jnp.bfloat16),
            pltpu.VMEM((16, D), jnp.bfloat16),
            pltpu.VMEM((HALO + 256, 256), jnp.bfloat16),
            pltpu.VMEM((136, 256), jnp.bfloat16),
            pltpu.VMEM((4, D, 256), jnp.bfloat16),
            pltpu.SemaphoreType.DMA((20,)),
        ],
        compiler_params=pltpu.CompilerParams(vmem_limit_bytes=49 * 2**20),
        cost_estimate=pl.CostEstimate(flops=1200000000, bytes_accessed=7000000, transcendentals=0),
    )(xs, *weights, taps)


def fold_kernel(got, mine, out, strip):
    total = f32(got[...]) + f32(mine[...])
    for i in range(4):
        out[i, :, :D] = bf(total[32 * i : 32 * (i + 1)])
    for t in range(2):
        for r in range(16):
            strip[16 * t + r : 16 * t + r + 1] = total[134 + t : 135 + t, 128 * r : 128 * (r + 1)]
    for i in range(4):
        out[i, :, D:] = bf(strip[...])


def folded(got, mine):
    return pl.pallas_call(
        fold_kernel,
        out_shape=jax.ShapeDtypeStruct((4, 32, D + 128), jnp.bfloat16),
        scratch_shapes=[pltpu.VMEM((32, 128), jnp.float32)],
        compiler_params=pltpu.CompilerParams(vmem_limit_bytes=6 * 2**20),
        cost_estimate=pl.CostEstimate(flops=1000000, bytes_accessed=2200000, transcendentals=0),
    )(got, mine)


def middle_kernel(got, kept, table, own, before, wide):
    total = f32(got[0]) + f32(got[1]) + f32(got[2]) + f32(got[3])
    wide[...] = jnp.zeros_like(wide)
    for t in range(2):
        for r in range(16):
            wide[6 + t : 7 + t, 128 * r : 128 * (r + 1)] = total[16 * t + r : 16 * t + r + 1, D:]
    gain, bias = table[0:1], table[2:3]
    own[...] = norm(kept[:32] + total[:, :D], gain, bias)
    before[...] = norm(kept[32:] + wide[...], gain, bias)


def middle(got, kept, table):
    shape = jax.ShapeDtypeStruct
    return pl.pallas_call(
        middle_kernel,
        out_shape=(shape((32, D), jnp.bfloat16), shape((8, D), jnp.bfloat16)),
        scratch_shapes=[pltpu.VMEM((8, D), jnp.float32)],
        compiler_params=pltpu.CompilerParams(vmem_limit_bytes=6 * 2**20),
        cost_estimate=pl.CostEstimate(flops=2000000, bytes_accessed=1200000, transcendentals=100),
    )(got, kept, table)


def rear_kernel(x, before, w, taps, sent, mine, held, acc, g, half, sems):
    core = lax.axis_index("core")
    first = jnp.logical_and(lax.axis_index("z") == 0, lax.axis_index("y") == 0)
    step = D // 4
    copies = [
        pltpu.make_async_copy(w.at[step * i : step * (i + 1)], held.at[step * i : step * (i + 1)], sems.at[i])
        for i in range(4)
    ]
    for copy in copies:
        copy.start()
    for i, copy in enumerate(copies):
        copy.wait()
        at = slice(step * i, step * (i + 1))
        for rows, source in ((slice(0, 8), before), (slice(8, 264), x)):
            part = jnp.dot(source[:, at], held[at, :768], preferred_element_type=jnp.float32)
            acc[rows] = part if i == 0 else acc[rows] + part
    u, outer, inner = (f32(bf(acc[:, 256 * i : 256 * (i + 1)])) for i in range(3))
    row = lax.broadcasted_iota(jnp.int32, u.shape, 0)
    z = jnp.where(jnp.logical_and(first, row < 8), 0.0, inner * u)
    conv = taps[2, 1:2] * z + taps[1, 1:2] * pltpu.roll(z, 1, 0) + taps[0, 1:2] * pltpu.roll(z, 2, 0)
    g[...] = bf((outer * conv)[8:])
    for target, which in ((sent, 1 - core), (mine, core)):
        for i in range(4):
            half[32 * i : 32 * (i + 1)] = g[pl.ds(pl.multiple_of(64 * i + 32 * which, 16), 32)]
        for n in range(4):
            at = slice(512 * n, 512 * (n + 1))
            part = lax.dot_general(
                half[...], held[at, 768:], (((1,), (1,)), ((), ())), preferred_element_type=jnp.float32
            )
            target[:, at] = part.astype(target.dtype)


def rear(x, before, w, taps):
    shape = jax.ShapeDtypeStruct
    return pl.pallas_call(
        rear_kernel,
        in_specs=[VMEM, VMEM, HBM, VMEM],
        out_specs=(VMEM, VMEM),
        out_shape=(shape((128, D), jnp.bfloat16),) * 2,
        scratch_shapes=[
            pltpu.VMEM((D, 1024), jnp.bfloat16),
            pltpu.VMEM((264, 768), jnp.float32),
            pltpu.VMEM((256, 256), jnp.bfloat16),
            pltpu.VMEM((128, 256), jnp.bfloat16),
            pltpu.SemaphoreType.DMA((4,)),
        ],
        compiler_params=pltpu.CompilerParams(vmem_limit_bytes=50 * 2**20),
        cost_estimate=pl.CostEstimate(flops=1200000000, bytes_accessed=7000000, transcendentals=0),
    )(x, before, w, taps)


def last_kernel(got, own, table, out):
    total = f32(got[0]) + f32(got[1]) + f32(got[2]) + f32(got[3])
    alpha = (2.0 * LAYERS) ** 0.25
    state = norm(alpha * f32(own[...]) + total, table[1:2], table[3:4])
    for i in range(8):
        out[i] = state[:, 256 * i : 256 * (i + 1)]


def last(got, own, table):
    return pl.pallas_call(
        last_kernel,
        out_shape=jax.ShapeDtypeStruct((8, 32, 256), jnp.bfloat16),
        compiler_params=pltpu.CompilerParams(vmem_limit_bytes=6 * 2**20),
        cost_estimate=pl.CostEstimate(flops=2000000, bytes_accessed=1200000, transcendentals=100),
    )(got, own, table)


def solution(mesh):
    mesh = Mesh(mesh.devices.reshape(8, 8, 4, 2), ("z", "y", "x", "core"))
    in_specs = (
        P(SP, TP),
        P(None, SP, TP),
        P(None, SP, TP),
        P(None, SP, TP),
        P(None, None, TP),
        P(None, TP, SP),
        P(None, TP),
        P(None, TP),
    )
    return jax.shard_map(shards, mesh=mesh, in_specs=in_specs, out_specs=P(SP, TP), check_vma=False)
```

```python
import jax
import jax.numpy as jnp
from jax import lax
from jax.experimental import pallas as pl
from jax.experimental.pallas import tpu as pltpu
from jax.sharding import Mesh, PartitionSpec as P


D = 2048
LAYERS = 2
TP = ("x", "core")
SP = ("z", "y")
HALO = 16
IN_UP, OUT_UP = 2.0**18, 2.0**14


def bf(x):
    return x.astype(jnp.bfloat16)


def f32(x):
    return x.astype(jnp.float32)


HBM = pl.BlockSpec(memory_space=pltpu.HBM)
VMEM = pl.BlockSpec(memory_space=pltpu.VMEM)


def pack_kernel(value, outer, inner, out_t, tokens, gain, bias, early, late, copies, held, rows, left, sems):
    fills = [pltpu.make_async_copy(w, held.at[i], sems.at[i]) for i, w in enumerate((value, outer, inner, out_t))]
    fills.append(pltpu.make_async_copy(gain, left.at[0:2], sems.at[4]))
    fills.append(pltpu.make_async_copy(bias, left.at[2:4], sems.at[5]))
    fills.append(pltpu.make_async_copy(tokens, rows.at[0:256], sems.at[6]))
    for copy in fills[4:] + fills[:4]:
        copy.start()
    fills[4].wait()
    fills[5].wait()
    rest = left[...]
    terms = []
    for _ in range(3):
        terms.append(f32(bf(rest)))
        rest = rest - terms[-1]
    terms.append(jnp.zeros_like(rest))
    rows[256:] = bf(jnp.concatenate(terms, axis=0))
    fills[6].wait()
    sends = [pltpu.make_async_copy(rows, copies.at[i, HALO : HALO + 272], sems.at[7 + i]) for i in range(8)]
    for copy in sends:
        copy.start()
    for i in range(4):
        at = slice(256 * i, 256 * (i + 1))
        fills[i].wait()
        early[:, at] = bf(f32(held[i, 0]) * (IN_UP if i < 3 else OUT_UP))
        late[:, at] = held[i, 1]
    for copy in sends:
        copy.wait()


HBM = pl.BlockSpec(memory_space=pltpu.HBM)
VMEM = pl.BlockSpec(memory_space=pltpu.VMEM)


def pack(value, outer, inner, out_t, tokens, gain, bias):
    shape = jax.ShapeDtypeStruct((32, 1024), jnp.bfloat16)
    return pl.pallas_call(
        pack_kernel,
        in_specs=[HBM] * 7,
        out_specs=(VMEM, VMEM, HBM),
        out_shape=(shape, shape, jax.ShapeDtypeStruct((8, 288, 256), jnp.bfloat16)),
        scratch_shapes=[
            pltpu.VMEM((4, 2, 32, 256), jnp.bfloat16),
            pltpu.VMEM((272, 256), jnp.bfloat16),
            pltpu.VMEM((4, 256), jnp.float32),
            pltpu.SemaphoreType.DMA((15,)),
        ],
        cost_estimate=pl.CostEstimate(flops=2000000, bytes_accessed=1700000, transcendentals=0),
    )(value, outer, inner, out_t, tokens, gain, bias)


def norm(pre, gain, bias):
    mean = jnp.mean(pre, axis=-1, keepdims=True)
    cent = pre - mean
    var = jnp.mean(cent * cent, axis=-1, keepdims=True)
    return bf(cent * lax.rsqrt(var + 1e-05) * gain + bias)


def shards(tokens, value, outer, inner, taps, out, gain, bias):
    taps = jnp.swapaxes(taps, 0, 1)
    halo = lax.ppermute(tokens[-HALO:], SP, [(i, i + 1) for i in range(63)])
    early, late, copies = pack(value, outer, inner, jnp.swapaxes(out, 1, 2), tokens, gain, bias)
    late = lax.all_gather(late, SP, axis=0, tiled=True)
    copies = lax.dynamic_update_slice(copies, jnp.broadcast_to(halo[None], (8, HALO, 256)), (0, 0, 0))
    everyone = lax.all_to_all(copies, TP, 0, 0, tiled=True)
    early = lax.all_gather(early.astype(jnp.float16), SP, axis=0, tiled=True)

    sent, mine, kept, table = front(everyone, [bf(early[:, 256 * i : 256 * (i + 1)]) for i in range(4)], taps)
    got = lax.ppermute(sent, "core", [(0, 1), (1, 0)])
    got = lax.all_to_all(folded(got, mine), "x", 0, 0, tiled=True)
    own, before = middle(got, kept, table)
    every = lax.all_gather(own.astype(jnp.float16), TP, axis=0, tiled=True)

    sent, mine = rear(bf(every), before, late, taps)
    got = lax.ppermute(sent, "core", [(0, 1), (1, 0)])
    got = lax.all_to_all(bf(f32(got) + f32(mine)).reshape(4, 32, D), "x", 0, 0, tiled=True)
    return lax.all_to_all(last(got, own, table), TP, 0, 0, tiled=True).reshape(256, 256)


def front_kernel(xs, w_u, w_outer, w_inner, w_out, taps, sent, mine, kept, table, x, tails, g, half, held, sems):
    core = lax.axis_index("core")
    tp = 2 * lax.axis_index("x") + core
    first = jnp.logical_and(lax.axis_index("z") == 0, lax.axis_index("y") == 0)
    rows = HALO + 256
    copies = [pltpu.make_async_copy(w_out, held, sems.at[0])]
    for j in range(8):
        at = slice(256 * j, 256 * (j + 1))
        copies.append(pltpu.make_async_copy(xs.at[j, 0:rows], x.at[:, at], sems.at[1 + j]))
        copies.append(pltpu.make_async_copy(xs.at[j, rows : rows + 16], tails.at[:, at], sems.at[9 + j]))
    for copy in copies[1:] + copies[:1]:
        copy.start()
    for copy in copies[1:]:
        copy.wait()
    tail = f32(tails[...])
    table[...] = tail[0:4] + tail[4:8] + tail[8:12]
    alpha = (2.0 * LAYERS) ** 0.25
    kept[:32] = alpha * f32(x[pl.ds(pl.multiple_of(HALO + 32 * tp, 16), 32)])
    kept[32:] = alpha * f32(x[HALO - 8 : HALO])
    product = lambda w: f32(bf(jnp.dot(x[...], w, preferred_element_type=jnp.float32) * (1.0 / IN_UP)))
    inner = product(w_inner[...])
    u = product(w_u[...])
    outer = product(w_outer[...])
    row = lax.broadcasted_iota(jnp.int32, u.shape, 0)
    z = jnp.where(jnp.logical_and(first, row < HALO), 0.0, inner * u)
    conv = taps[2, 0:1] * z + taps[1, 0:1] * pltpu.roll(z, 1, 0) + taps[0, 0:1] * pltpu.roll(z, 2, 0)
    g[...] = bf(outer * conv)
    half[128:] = g[HALO - 8 : HALO]
    copies[0].wait()
    for target, which in ((sent, 1 - core), (mine, core)):
        for i in range(4):
            half[32 * i : 32 * (i + 1)] = g[pl.ds(pl.multiple_of(HALO + 64 * i + 32 * which, 16), 32)]
        for n in range(4):
            at = slice(512 * n, 512 * (n + 1))
            part = lax.dot_general(
                half[...], held[at], (((1,), (1,)), ((), ())), preferred_element_type=jnp.float32
            ) * (1.0 / OUT_UP)
            target[:, at] = part.astype(target.dtype)


def front(xs, weights, taps):
    shape = jax.ShapeDtypeStruct
    return pl.pallas_call(
        front_kernel,
        in_specs=[HBM, VMEM, VMEM, VMEM, HBM, VMEM],
        out_specs=(VMEM,) * 4,
        out_shape=(
            shape((136, D), jnp.bfloat16),
            shape((136, D), jnp.bfloat16),
            shape((40, D), jnp.float32),
            shape((4, D), jnp.float32),
        ),
        scratch_shapes=[
            pltpu.VMEM((HALO + 256, D), jnp.bfloat16),
            pltpu.VMEM((16, D), jnp.bfloat16),
            pltpu.VMEM((HALO + 256, 256), jnp.bfloat16),
            pltpu.VMEM((136, 256), jnp.bfloat16),
            pltpu.VMEM((D, 256), jnp.bfloat16),
            pltpu.SemaphoreType.DMA((17,)),
        ],
        compiler_params=pltpu.CompilerParams(vmem_limit_bytes=49 * 2**20),
        cost_estimate=pl.CostEstimate(flops=1200000000, bytes_accessed=7000000, transcendentals=0),
    )(xs, *weights, taps)


def fold_kernel(got, mine, out, strip):
    total = f32(got[...]) + f32(mine[...])
    for i in range(4):
        out[i, :, :D] = bf(total[32 * i : 32 * (i + 1)])
    for t in range(2):
        for r in range(16):
            strip[16 * t + r : 16 * t + r + 1] = total[134 + t : 135 + t, 128 * r : 128 * (r + 1)]
    for i in range(4):
        out[i, :, D:] = bf(strip[...])


def folded(got, mine):
    return pl.pallas_call(
        fold_kernel,
        out_shape=jax.ShapeDtypeStruct((4, 32, D + 128), jnp.bfloat16),
        scratch_shapes=[pltpu.VMEM((32, 128), jnp.float32)],
        compiler_params=pltpu.CompilerParams(vmem_limit_bytes=6 * 2**20),
        cost_estimate=pl.CostEstimate(flops=1000000, bytes_accessed=2200000, transcendentals=0),
    )(got, mine)


def middle_kernel(got, kept, table, own, before, wide):
    total = f32(got[0]) + f32(got[1]) + f32(got[2]) + f32(got[3])
    wide[...] = jnp.zeros_like(wide)
    for t in range(2):
        for r in range(16):
            wide[6 + t : 7 + t, 128 * r : 128 * (r + 1)] = total[16 * t + r : 16 * t + r + 1, D:]
    gain, bias = table[0:1], table[2:3]
    own[...] = norm(kept[:32] + total[:, :D], gain, bias)
    before[...] = norm(kept[32:] + wide[...], gain, bias)


def middle(got, kept, table):
    shape = jax.ShapeDtypeStruct
    return pl.pallas_call(
        middle_kernel,
        out_shape=(shape((32, D), jnp.bfloat16), shape((8, D), jnp.bfloat16)),
        scratch_shapes=[pltpu.VMEM((8, D), jnp.float32)],
        compiler_params=pltpu.CompilerParams(vmem_limit_bytes=6 * 2**20),
        cost_estimate=pl.CostEstimate(flops=2000000, bytes_accessed=1200000, transcendentals=100),
    )(got, kept, table)


def rear_kernel(x, before, w, taps, sent, mine, held, acc, g, half, sems):
    core = lax.axis_index("core")
    first = jnp.logical_and(lax.axis_index("z") == 0, lax.axis_index("y") == 0)
    step = D // 4
    copies = [
        pltpu.make_async_copy(w.at[at, 0:768], held.at[at, 0:768], sems.at[i])
        for i, at in enumerate(pl.ds(step * i, step) for i in range(4))
    ]
    copies.append(pltpu.make_async_copy(w.at[:, 768:1024], held.at[:, 768:1024], sems.at[4]))
    for copy in copies:
        copy.start()
    for i in range(4):
        copies[i].wait()
        at = slice(step * i, step * (i + 1))
        for rows, source in ((slice(0, 8), before), (slice(8, 264), x)):
            part = jnp.dot(source[:, at], held[at, :768], preferred_element_type=jnp.float32)
            acc[rows] = part if i == 0 else acc[rows] + part
    u, outer, inner = (f32(bf(acc[:, 256 * i : 256 * (i + 1)])) for i in range(3))
    row = lax.broadcasted_iota(jnp.int32, u.shape, 0)
    z = jnp.where(jnp.logical_and(first, row < 8), 0.0, inner * u)
    conv = taps[2, 1:2] * z + taps[1, 1:2] * pltpu.roll(z, 1, 0) + taps[0, 1:2] * pltpu.roll(z, 2, 0)
    g[...] = bf((outer * conv)[8:])
    copies[4].wait()
    for target, which in ((sent, 1 - core), (mine, core)):
        for i in range(4):
            half[32 * i : 32 * (i + 1)] = g[pl.ds(pl.multiple_of(64 * i + 32 * which, 16), 32)]
        for n in range(4):
            at = slice(512 * n, 512 * (n + 1))
            part = lax.dot_general(
                half[...], held[at, 768:], (((1,), (1,)), ((), ())), preferred_element_type=jnp.float32
            )
            target[:, at] = part.astype(target.dtype)


def rear(x, before, w, taps):
    shape = jax.ShapeDtypeStruct
    return pl.pallas_call(
        rear_kernel,
        in_specs=[VMEM, VMEM, HBM, VMEM],
        out_specs=(VMEM, VMEM),
        out_shape=(shape((128, D), jnp.bfloat16),) * 2,
        scratch_shapes=[
            pltpu.VMEM((D, 1024), jnp.bfloat16),
            pltpu.VMEM((264, 768), jnp.float32),
            pltpu.VMEM((256, 256), jnp.bfloat16),
            pltpu.VMEM((128, 256), jnp.bfloat16),
            pltpu.SemaphoreType.DMA((5,)),
        ],
        compiler_params=pltpu.CompilerParams(vmem_limit_bytes=50 * 2**20),
        cost_estimate=pl.CostEstimate(flops=1200000000, bytes_accessed=7000000, transcendentals=0),
    )(x, before, w, taps)


def last_kernel(got, own, table, out):
    total = f32(got[0]) + f32(got[1]) + f32(got[2]) + f32(got[3])
    alpha = (2.0 * LAYERS) ** 0.25
    state = norm(alpha * f32(own[...]) + total, table[1:2], table[3:4])
    for i in range(8):
        out[i] = state[:, 256 * i : 256 * (i + 1)]


def last(got, own, table):
    return pl.pallas_call(
        last_kernel,
        out_shape=jax.ShapeDtypeStruct((8, 32, 256), jnp.bfloat16),
        compiler_params=pltpu.CompilerParams(vmem_limit_bytes=6 * 2**20),
        cost_estimate=pl.CostEstimate(flops=2000000, bytes_accessed=1200000, transcendentals=100),
    )(got, own, table)


def solution(mesh):
    mesh = Mesh(mesh.devices.reshape(8, 8, 4, 2), ("z", "y", "x", "core"))
    in_specs = (
        P(SP, TP),
        P(None, SP, TP),
        P(None, SP, TP),
        P(None, SP, TP),
        P(None, None, TP),
        P(None, TP, SP),
        P(None, TP),
        P(None, TP),
    )
    return jax.shard_map(shards, mesh=mesh, in_specs=in_specs, out_specs=P(SP, TP), check_vma=False)
```

```python
import functools

import jax
import jax.numpy as jnp
from jax import lax
from jax.experimental import pallas as pl
from jax.experimental.pallas import tpu as pltpu
from jax.sharding import Mesh, PartitionSpec as P


D = 2048
LAYERS = 2
TP = ("x", "core")
SP = ("z", "y")
HALO = 16
IN_UP, OUT_UP = 2.0**18, 2.0**14


def bf(x):
    return x.astype(jnp.bfloat16)


def f32(x):
    return x.astype(jnp.float32)


HBM = pl.BlockSpec(memory_space=pltpu.HBM)
VMEM = pl.BlockSpec(memory_space=pltpu.VMEM)


def pack_kernel(value, outer, inner, out_t, tokens, gain, bias, early, late, copies, held, rows, left, sems):
    fills = [pltpu.make_async_copy(w, held.at[i], sems.at[i]) for i, w in enumerate((value, outer, inner, out_t))]
    fills.append(pltpu.make_async_copy(gain, left.at[0:2], sems.at[4]))
    fills.append(pltpu.make_async_copy(bias, left.at[2:4], sems.at[5]))
    fills.append(pltpu.make_async_copy(tokens, rows.at[0:256], sems.at[6]))
    for copy in fills[4:] + fills[:4]:
        copy.start()
    fills[4].wait()
    fills[5].wait()
    rest = left[...]
    terms = []
    for _ in range(3):
        terms.append(f32(bf(rest)))
        rest = rest - terms[-1]
    terms.append(jnp.zeros_like(rest))
    rows[256:] = bf(jnp.concatenate(terms, axis=0))
    fills[6].wait()
    sends = [pltpu.make_async_copy(rows, copies.at[i, HALO : HALO + 272], sems.at[7 + i]) for i in range(8)]
    for copy in sends:
        copy.start()
    for i in range(4):
        at = slice(256 * i, 256 * (i + 1))
        fills[i].wait()
        early[:, at] = bf(f32(held[i, 0]) * (IN_UP if i < 3 else OUT_UP))
        late[:, at] = held[i, 1]
    for copy in sends:
        copy.wait()


HBM = pl.BlockSpec(memory_space=pltpu.HBM)
VMEM = pl.BlockSpec(memory_space=pltpu.VMEM)


def pack(value, outer, inner, out_t, tokens, gain, bias):
    shape = jax.ShapeDtypeStruct((32, 1024), jnp.bfloat16)
    return pl.pallas_call(
        pack_kernel,
        in_specs=[HBM] * 7,
        out_specs=(VMEM, VMEM, HBM),
        out_shape=(shape, shape, jax.ShapeDtypeStruct((8, 288, 256), jnp.bfloat16)),
        scratch_shapes=[
            pltpu.VMEM((4, 2, 32, 256), jnp.bfloat16),
            pltpu.VMEM((272, 256), jnp.bfloat16),
            pltpu.VMEM((4, 256), jnp.float32),
            pltpu.SemaphoreType.DMA((15,)),
        ],
        cost_estimate=pl.CostEstimate(flops=2000000, bytes_accessed=1700000, transcendentals=0),
    )(value, outer, inner, out_t, tokens, gain, bias)


def norm(pre, gain, bias):
    mean = jnp.mean(pre, axis=-1, keepdims=True)
    cent = pre - mean
    var = jnp.mean(cent * cent, axis=-1, keepdims=True)
    return bf(cent * lax.rsqrt(var + 1e-05) * gain + bias)


def shards(tokens, value, outer, inner, taps, out, gain, bias):
    taps = jnp.swapaxes(taps, 0, 1)
    halo = lax.ppermute(tokens[-HALO:], SP, [(i, i + 1) for i in range(63)])
    early, late, copies = pack(value, outer, inner, jnp.swapaxes(out, 1, 2), tokens, gain, bias)
    late = lax.all_gather(late, SP, axis=0, tiled=True)
    copies = lax.dynamic_update_slice(copies, jnp.broadcast_to(halo[None], (8, HALO, 256)), (0, 0, 0))
    everyone = lax.all_to_all(copies, TP, 0, 0, tiled=True)
    early = lax.all_gather(early.astype(jnp.float16), SP, axis=0, tiled=True)

    weights = [bf(early[:, 256 * i : 256 * (i + 1)]) for i in range(4)]
    sent, half, kept, table = front(everyone, weights, taps)
    got = lax.ppermute(sent, "core", [(0, 1), (1, 0)])
    mine = own_product(half, weights[3], 0, 1.0 / OUT_UP, 49)
    got = lax.all_to_all(folded(got, mine), "x", 0, 0, tiled=True)
    own, before = middle(got, kept, table)
    every = lax.all_gather(own.astype(jnp.float16), TP, axis=0, tiled=True)

    sent, half = rear(bf(every), before, late, taps)
    got = lax.ppermute(sent, "core", [(0, 1), (1, 0)])
    mine = own_product(half, late, 768, 1.0, 52)
    got = lax.all_to_all(bf(f32(got) + f32(mine)).reshape(4, 32, D), "x", 0, 0, tiled=True)
    return lax.all_to_all(last(got, own, table), TP, 0, 0, tiled=True).reshape(256, 256)


def out_product(rows, w_out, down, target):
    for n in range(4):
        at = slice(512 * n, 512 * (n + 1))
        part = lax.dot_general(rows, w_out[at], (((1,), (1,)), ((), ())), preferred_element_type=jnp.float32)
        target[:, at] = bf(part * down)


def front_kernel(xs, w_u, w_outer, w_inner, w_out, taps, sent, own, kept, table, x, tails, g, half, held, sems):
    core = lax.axis_index("core")
    tp = 2 * lax.axis_index("x") + core
    first = jnp.logical_and(lax.axis_index("z") == 0, lax.axis_index("y") == 0)
    rows = HALO + 256
    blocks, ends = [], []
    for j in range(8):
        at = slice(256 * j, 256 * (j + 1))
        blocks.append(pltpu.make_async_copy(xs.at[j, 0:rows], x.at[:, at], sems.at[j]))
        ends.append(pltpu.make_async_copy(xs.at[j, rows : rows + 16], tails.at[:, at], sems.at[8 + j]))
    weight = pltpu.make_async_copy(w_out, held, sems.at[16])
    for copy in blocks + [weight] + ends:
        copy.start()
    sums = [0.0, 0.0, 0.0]
    for part in range(2):
        for copy in blocks[4 * part : 4 * (part + 1)]:
            copy.wait()
        at = slice(1024 * part, 1024 * (part + 1))
        for i, w in enumerate((w_u, w_outer, w_inner)):
            sums[i] = sums[i] + jnp.dot(x[:, at], w[at], preferred_element_type=jnp.float32)
    u, outer, inner = (f32(bf(total * (1.0 / IN_UP))) for total in sums)
    row = lax.broadcasted_iota(jnp.int32, u.shape, 0)
    z = jnp.where(jnp.logical_and(first, row < HALO), 0.0, inner * u)
    conv = taps[2, 0:1] * z + taps[1, 0:1] * pltpu.roll(z, 1, 0) + taps[0, 0:1] * pltpu.roll(z, 2, 0)
    g[...] = bf(outer * conv)
    for target, which in ((half, 1 - core), (own, core)):
        target[128:] = g[HALO - 8 : HALO]
        for i in range(4):
            target[32 * i : 32 * (i + 1)] = g[pl.ds(pl.multiple_of(HALO + 64 * i + 32 * which, 16), 32)]
    weight.wait()
    out_product(half[...], held, 1.0 / OUT_UP, sent)
    alpha = (2.0 * LAYERS) ** 0.25
    kept[:32] = alpha * f32(x[pl.ds(pl.multiple_of(HALO + 32 * tp, 16), 32)])
    kept[32:] = alpha * f32(x[HALO - 8 : HALO])
    for copy in ends:
        copy.wait()
    tail = f32(tails[...])
    table[...] = tail[0:4] + tail[4:8] + tail[8:12]


def front(xs, weights, taps):
    shape = jax.ShapeDtypeStruct
    return pl.pallas_call(
        front_kernel,
        in_specs=[HBM, VMEM, VMEM, VMEM, HBM, VMEM],
        out_specs=(VMEM,) * 4,
        out_shape=(
            shape((136, D), jnp.bfloat16),
            shape((136, 256), jnp.bfloat16),
            shape((40, D), jnp.float32),
            shape((4, D), jnp.float32),
        ),
        scratch_shapes=[
            pltpu.VMEM((HALO + 256, D), jnp.bfloat16),
            pltpu.VMEM((16, D), jnp.bfloat16),
            pltpu.VMEM((HALO + 256, 256), jnp.bfloat16),
            pltpu.VMEM((136, 256), jnp.bfloat16),
            pltpu.VMEM((D, 256), jnp.bfloat16),
            pltpu.SemaphoreType.DMA((17,)),
        ],
        compiler_params=pltpu.CompilerParams(vmem_limit_bytes=49 * 2**20),
        cost_estimate=pl.CostEstimate(flops=1200000000, bytes_accessed=7000000, transcendentals=0),
    )(xs, *weights, taps)


def own_kernel(column, down, rows, w, mine, held, sem):
    copy = pltpu.make_async_copy(w.at[:, column : column + 256], held, sem.at[0])
    copy.start()
    copy.wait()
    out_product(rows[...], held, down, mine)


def own_product(rows, w, column, down, limit):
    return pl.pallas_call(
        functools.partial(own_kernel, column, down),
        in_specs=[VMEM, HBM],
        out_specs=VMEM,
        out_shape=jax.ShapeDtypeStruct((rows.shape[0], D), jnp.bfloat16),
        scratch_shapes=[pltpu.VMEM((D, 256), jnp.bfloat16), pltpu.SemaphoreType.DMA((1,))],
        compiler_params=pltpu.CompilerParams(vmem_limit_bytes=limit * 2**20),
        cost_estimate=pl.CostEstimate(flops=800000000, bytes_accessed=2000000, transcendentals=0),
    )(rows, w)


def fold_kernel(got, mine, out, strip):
    total = f32(got[...]) + f32(mine[...])
    for i in range(4):
        out[i, :, :D] = bf(total[32 * i : 32 * (i + 1)])
    for t in range(2):
        for r in range(16):
            strip[16 * t + r : 16 * t + r + 1] = total[134 + t : 135 + t, 128 * r : 128 * (r + 1)]
    for i in range(4):
        out[i, :, D:] = bf(strip[...])


def folded(got, mine):
    return pl.pallas_call(
        fold_kernel,
        out_shape=jax.ShapeDtypeStruct((4, 32, D + 128), jnp.bfloat16),
        scratch_shapes=[pltpu.VMEM((32, 128), jnp.float32)],
        compiler_params=pltpu.CompilerParams(vmem_limit_bytes=6 * 2**20),
        cost_estimate=pl.CostEstimate(flops=1000000, bytes_accessed=2200000, transcendentals=0),
    )(got, mine)


def middle_kernel(got, kept, table, own, before, wide):
    total = f32(got[0]) + f32(got[1]) + f32(got[2]) + f32(got[3])
    wide[...] = jnp.zeros_like(wide)
    for t in range(2):
        for r in range(16):
            wide[6 + t : 7 + t, 128 * r : 128 * (r + 1)] = total[16 * t + r : 16 * t + r + 1, D:]
    gain, bias = table[0:1], table[2:3]
    own[...] = norm(kept[:32] + total[:, :D], gain, bias)
    before[...] = norm(kept[32:] + wide[...], gain, bias)


def middle(got, kept, table):
    shape = jax.ShapeDtypeStruct
    return pl.pallas_call(
        middle_kernel,
        out_shape=(shape((32, D), jnp.bfloat16), shape((8, D), jnp.bfloat16)),
        scratch_shapes=[pltpu.VMEM((8, D), jnp.float32)],
        compiler_params=pltpu.CompilerParams(vmem_limit_bytes=6 * 2**20),
        cost_estimate=pl.CostEstimate(flops=2000000, bytes_accessed=1200000, transcendentals=100),
    )(got, kept, table)


def rear_kernel(x, before, w, taps, sent, own, held, acc, g, half, sems):
    core = lax.axis_index("core")
    first = jnp.logical_and(lax.axis_index("z") == 0, lax.axis_index("y") == 0)
    step = D // 4
    copies = [
        pltpu.make_async_copy(w.at[at, 0:768], held.at[at, 0:768], sems.at[i])
        for i, at in enumerate(pl.ds(step * i, step) for i in range(4))
    ]
    copies.append(pltpu.make_async_copy(w.at[:, 768:1024], held.at[:, 768:1024], sems.at[4]))
    for copy in copies:
        copy.start()
    for i in range(4):
        copies[i].wait()
        at = slice(step * i, step * (i + 1))
        for rows, source in ((slice(0, 8), before), (slice(8, 264), x)):
            part = jnp.dot(source[:, at], held[at, :768], preferred_element_type=jnp.float32)
            acc[rows] = part if i == 0 else acc[rows] + part
    u, outer, inner = (f32(bf(acc[:, 256 * i : 256 * (i + 1)])) for i in range(3))
    row = lax.broadcasted_iota(jnp.int32, u.shape, 0)
    z = jnp.where(jnp.logical_and(first, row < 8), 0.0, inner * u)
    conv = taps[2, 1:2] * z + taps[1, 1:2] * pltpu.roll(z, 1, 0) + taps[0, 1:2] * pltpu.roll(z, 2, 0)
    g[...] = bf((outer * conv)[8:])
    for target, which in ((half, 1 - core), (own, core)):
        for i in range(4):
            target[32 * i : 32 * (i + 1)] = g[pl.ds(pl.multiple_of(64 * i + 32 * which, 16), 32)]
    copies[4].wait()
    out_product(half[...], held.at[:, 768:1024], 1.0, sent)


def rear(x, before, w, taps):
    shape = jax.ShapeDtypeStruct
    return pl.pallas_call(
        rear_kernel,
        in_specs=[VMEM, VMEM, HBM, VMEM],
        out_specs=(VMEM, VMEM),
        out_shape=(shape((128, D), jnp.bfloat16), shape((128, 256), jnp.bfloat16)),
        scratch_shapes=[
            pltpu.VMEM((D, 1024), jnp.bfloat16),
            pltpu.VMEM((264, 768), jnp.float32),
            pltpu.VMEM((256, 256), jnp.bfloat16),
            pltpu.VMEM((128, 256), jnp.bfloat16),
            pltpu.SemaphoreType.DMA((5,)),
        ],
        compiler_params=pltpu.CompilerParams(vmem_limit_bytes=50 * 2**20),
        cost_estimate=pl.CostEstimate(flops=1200000000, bytes_accessed=7000000, transcendentals=0),
    )(x, before, w, taps)


def last_kernel(got, own, table, out):
    total = f32(got[0]) + f32(got[1]) + f32(got[2]) + f32(got[3])
    alpha = (2.0 * LAYERS) ** 0.25
    state = norm(alpha * f32(own[...]) + total, table[1:2], table[3:4])
    for i in range(8):
        out[i] = state[:, 256 * i : 256 * (i + 1)]


def last(got, own, table):
    return pl.pallas_call(
        last_kernel,
        out_shape=jax.ShapeDtypeStruct((8, 32, 256), jnp.bfloat16),
        compiler_params=pltpu.CompilerParams(vmem_limit_bytes=6 * 2**20),
        cost_estimate=pl.CostEstimate(flops=2000000, bytes_accessed=1200000, transcendentals=100),
    )(got, own, table)


def solution(mesh):
    mesh = Mesh(mesh.devices.reshape(8, 8, 4, 2), ("z", "y", "x", "core"))
    in_specs = (
        P(SP, TP),
        P(None, SP, TP),
        P(None, SP, TP),
        P(None, SP, TP),
        P(None, None, TP),
        P(None, TP, SP),
        P(None, TP),
        P(None, TP),
    )
    return jax.shard_map(shards, mesh=mesh, in_specs=in_specs, out_specs=P(SP, TP), check_vma=False)
```

```python
import functools

import jax
import jax.numpy as jnp
from jax import lax
from jax.experimental import pallas as pl
from jax.experimental.pallas import tpu as pltpu
from jax.sharding import Mesh, PartitionSpec as P


D = 2048
LAYERS = 2
TP = ("x", "core")
SP = ("z", "y")
HALO = 16
IN_UP, OUT_UP = 2.0**18, 2.0**14


def bf(x):
    return x.astype(jnp.bfloat16)


def f32(x):
    return x.astype(jnp.float32)


HBM = pl.BlockSpec(memory_space=pltpu.HBM)
VMEM = pl.BlockSpec(memory_space=pltpu.VMEM)


def pack_kernel(value, outer, inner, out_t, tokens, gain, bias, early, late, copies, held, rows, left, sems):
    fills = [pltpu.make_async_copy(w, held.at[i], sems.at[i]) for i, w in enumerate((value, outer, inner, out_t))]
    fills.append(pltpu.make_async_copy(gain, left.at[0:2], sems.at[4]))
    fills.append(pltpu.make_async_copy(bias, left.at[2:4], sems.at[5]))
    fills.append(pltpu.make_async_copy(tokens, rows.at[0:256], sems.at[6]))
    for copy in fills[4:] + fills[:4]:
        copy.start()
    fills[4].wait()
    fills[5].wait()
    rest = left[...]
    terms = []
    for _ in range(3):
        terms.append(f32(bf(rest)))
        rest = rest - terms[-1]
    terms.append(jnp.zeros_like(rest))
    rows[256:] = bf(jnp.concatenate(terms, axis=0))
    fills[6].wait()
    sends = [pltpu.make_async_copy(rows, copies.at[i, HALO : HALO + 272], sems.at[7 + i]) for i in range(8)]
    for copy in sends:
        copy.start()
    for i in range(4):
        at = slice(256 * i, 256 * (i + 1))
        fills[i].wait()
        early[:, at] = bf(f32(held[i, 0]) * (IN_UP if i < 3 else OUT_UP))
        late[:, at] = held[i, 1]
    for copy in sends:
        copy.wait()


HBM = pl.BlockSpec(memory_space=pltpu.HBM)
VMEM = pl.BlockSpec(memory_space=pltpu.VMEM)


def pack(value, outer, inner, out_t, tokens, gain, bias):
    shape = jax.ShapeDtypeStruct((32, 1024), jnp.bfloat16)
    return pl.pallas_call(
        pack_kernel,
        in_specs=[HBM] * 7,
        out_specs=(VMEM, VMEM, HBM),
        out_shape=(shape, shape, jax.ShapeDtypeStruct((8, 288, 256), jnp.bfloat16)),
        scratch_shapes=[
            pltpu.VMEM((4, 2, 32, 256), jnp.bfloat16),
            pltpu.VMEM((272, 256), jnp.bfloat16),
            pltpu.VMEM((4, 256), jnp.float32),
            pltpu.SemaphoreType.DMA((15,)),
        ],
        cost_estimate=pl.CostEstimate(flops=2000000, bytes_accessed=1700000, transcendentals=0),
    )(value, outer, inner, out_t, tokens, gain, bias)


def norm(pre, gain, bias):
    mean = jnp.mean(pre, axis=-1, keepdims=True)
    cent = pre - mean
    var = jnp.mean(cent * cent, axis=-1, keepdims=True)
    return bf(cent * lax.rsqrt(var + 1e-05) * gain + bias)


def shards(tokens, value, outer, inner, taps, out, gain, bias):
    taps = jnp.swapaxes(taps, 0, 1)
    halo = lax.ppermute(tokens[-HALO:], SP, [(i, i + 1) for i in range(63)])
    early, late, copies = pack(value, outer, inner, jnp.swapaxes(out, 1, 2), tokens, gain, bias)
    late = lax.all_gather(late, SP, axis=0, tiled=True)
    copies = lax.dynamic_update_slice(copies, jnp.broadcast_to(halo[None], (8, HALO, 256)), (0, 0, 0))
    everyone = lax.all_to_all(copies, TP, 0, 0, tiled=True)
    early = lax.all_gather(early.astype(jnp.float16), SP, axis=0, tiled=True)

    weights = [bf(early[:, 256 * i : 256 * (i + 1)]) for i in range(4)]
    sent, half = front(everyone, weights, taps)
    got = lax.ppermute(sent, "core", [(0, 1), (1, 0)])
    mine, kept, table = aside(half, weights[3], everyone)
    got = lax.all_to_all(folded(got, mine), "x", 0, 0, tiled=True)
    own, before = middle(got, kept, table)
    every = lax.all_gather(own.astype(jnp.float16), TP, axis=0, tiled=True)

    sent, half = rear(bf(every), before, late, taps)
    got = lax.ppermute(sent, "core", [(0, 1), (1, 0)])
    mine = own_product(half, late, 768, 1.0, 52)
    got = lax.all_to_all(bf(f32(got) + f32(mine)).reshape(4, 32, D), "x", 0, 0, tiled=True)
    return lax.all_to_all(last(got, own, table), TP, 0, 0, tiled=True).reshape(256, 256)


def out_product(rows, w_out, down, target):
    for n in range(4):
        at = slice(512 * n, 512 * (n + 1))
        part = lax.dot_general(rows, w_out[at], (((1,), (1,)), ((), ())), preferred_element_type=jnp.float32)
        target[:, at] = bf(part * down)


def front_kernel(xs, w_u, w_outer, w_inner, w_out, taps, sent, own, x, g, half, held, sems):
    core = lax.axis_index("core")
    first = jnp.logical_and(lax.axis_index("z") == 0, lax.axis_index("y") == 0)
    rows = HALO + 256
    blocks = [
        pltpu.make_async_copy(xs.at[j, 0:rows], x.at[:, 256 * j : 256 * (j + 1)], sems.at[j]) for j in range(8)
    ]
    weight = pltpu.make_async_copy(w_out, held, sems.at[8])
    for copy in blocks:
        copy.start()
    sums = [0.0, 0.0, 0.0]
    for part in range(2):
        for copy in blocks[4 * part : 4 * (part + 1)]:
            copy.wait()
        if part == 1:
            weight.start()
        at = slice(1024 * part, 1024 * (part + 1))
        for i, w in enumerate((w_u, w_outer, w_inner)):
            sums[i] = sums[i] + jnp.dot(x[:, at], w[at], preferred_element_type=jnp.float32)
    u, outer, inner = (f32(bf(total * (1.0 / IN_UP))) for total in sums)
    row = lax.broadcasted_iota(jnp.int32, u.shape, 0)
    z = jnp.where(jnp.logical_and(first, row < HALO), 0.0, inner * u)
    conv = taps[2, 0:1] * z + taps[1, 0:1] * pltpu.roll(z, 1, 0) + taps[0, 0:1] * pltpu.roll(z, 2, 0)
    g[...] = bf(outer * conv)
    for target, which in ((half, 1 - core), (own, core)):
        target[128:] = g[HALO - 8 : HALO]
        for i in range(4):
            target[32 * i : 32 * (i + 1)] = g[pl.ds(pl.multiple_of(HALO + 64 * i + 32 * which, 16), 32)]
    weight.wait()
    out_product(half[...], held, 1.0 / OUT_UP, sent)


def front(xs, weights, taps):
    shape = jax.ShapeDtypeStruct
    return pl.pallas_call(
        front_kernel,
        in_specs=[HBM, VMEM, VMEM, VMEM, HBM, VMEM],
        out_specs=(VMEM,) * 2,
        out_shape=(shape((136, D), jnp.bfloat16), shape((136, 256), jnp.bfloat16)),
        scratch_shapes=[
            pltpu.VMEM((HALO + 256, D), jnp.bfloat16),
            pltpu.VMEM((HALO + 256, 256), jnp.bfloat16),
            pltpu.VMEM((136, 256), jnp.bfloat16),
            pltpu.VMEM((D, 256), jnp.bfloat16),
            pltpu.SemaphoreType.DMA((9,)),
        ],
        compiler_params=pltpu.CompilerParams(vmem_limit_bytes=50 * 2**20),
        cost_estimate=pl.CostEstimate(flops=1200000000, bytes_accessed=7000000, transcendentals=0),
    )(xs, *weights, taps)


def aside_kernel(rows, w, xs, mine, kept, table, held, x, tails, sems):
    tp = 2 * lax.axis_index("x") + lax.axis_index("core")
    weight = pltpu.make_async_copy(w, held, sems.at[0])
    weight.start()
    copies = []
    for j in range(8):
        at = slice(256 * j, 256 * (j + 1))
        start = pl.multiple_of(HALO + 32 * tp, 16)
        copies.append(pltpu.make_async_copy(xs.at[j, pl.ds(start, 32)], x.at[0:32, at], sems.at[1 + j]))
        copies.append(pltpu.make_async_copy(xs.at[j, HALO - 8 : HALO], x.at[32:40, at], sems.at[9 + j]))
        copies.append(pltpu.make_async_copy(xs.at[j, HALO + 256 : HALO + 272], tails.at[:, at], sems.at[17 + j]))
    for copy in copies:
        copy.start()
    weight.wait()
    out_product(rows[...], held, 1.0 / OUT_UP, mine)
    for copy in copies:
        copy.wait()
    kept[...] = (2.0 * LAYERS) ** 0.25 * f32(x[...])
    tail = f32(tails[...])
    table[...] = tail[0:4] + tail[4:8] + tail[8:12]


def aside(rows, w, xs):
    shape = jax.ShapeDtypeStruct
    return pl.pallas_call(
        aside_kernel,
        in_specs=[VMEM, HBM, HBM],
        out_specs=(VMEM,) * 3,
        out_shape=(shape((136, D), jnp.bfloat16), shape((40, D), jnp.float32), shape((4, D), jnp.float32)),
        scratch_shapes=[
            pltpu.VMEM((D, 256), jnp.bfloat16),
            pltpu.VMEM((40, D), jnp.bfloat16),
            pltpu.VMEM((16, D), jnp.bfloat16),
            pltpu.SemaphoreType.DMA((25,)),
        ],
        compiler_params=pltpu.CompilerParams(vmem_limit_bytes=52 * 2**20),
        cost_estimate=pl.CostEstimate(flops=800000000, bytes_accessed=2000000, transcendentals=0),
    )(rows, w, xs)


def own_kernel(column, down, rows, w, mine, held, sem):
    copy = pltpu.make_async_copy(w.at[:, column : column + 256], held, sem.at[0])
    copy.start()
    copy.wait()
    out_product(rows[...], held, down, mine)


def own_product(rows, w, column, down, limit):
    return pl.pallas_call(
        functools.partial(own_kernel, column, down),
        in_specs=[VMEM, HBM],
        out_specs=VMEM,
        out_shape=jax.ShapeDtypeStruct((rows.shape[0], D), jnp.bfloat16),
        scratch_shapes=[pltpu.VMEM((D, 256), jnp.bfloat16), pltpu.SemaphoreType.DMA((1,))],
        compiler_params=pltpu.CompilerParams(vmem_limit_bytes=limit * 2**20),
        cost_estimate=pl.CostEstimate(flops=800000000, bytes_accessed=2000000, transcendentals=0),
    )(rows, w)


def fold_kernel(got, mine, out, strip):
    total = f32(got[...]) + f32(mine[...])
    for i in range(4):
        out[i, :, :D] = bf(total[32 * i : 32 * (i + 1)])
    for t in range(2):
        for r in range(16):
            strip[16 * t + r : 16 * t + r + 1] = total[134 + t : 135 + t, 128 * r : 128 * (r + 1)]
    for i in range(4):
        out[i, :, D:] = bf(strip[...])


def folded(got, mine):
    return pl.pallas_call(
        fold_kernel,
        out_shape=jax.ShapeDtypeStruct((4, 32, D + 128), jnp.bfloat16),
        scratch_shapes=[pltpu.VMEM((32, 128), jnp.float32)],
        compiler_params=pltpu.CompilerParams(vmem_limit_bytes=6 * 2**20),
        cost_estimate=pl.CostEstimate(flops=1000000, bytes_accessed=2200000, transcendentals=0),
    )(got, mine)


def middle_kernel(got, kept, table, own, before, wide):
    total = f32(got[0]) + f32(got[1]) + f32(got[2]) + f32(got[3])
    wide[...] = jnp.zeros_like(wide)
    for t in range(2):
        for r in range(16):
            wide[6 + t : 7 + t, 128 * r : 128 * (r + 1)] = total[16 * t + r : 16 * t + r + 1, D:]
    gain, bias = table[0:1], table[2:3]
    own[...] = norm(kept[:32] + total[:, :D], gain, bias)
    before[...] = norm(kept[32:] + wide[...], gain, bias)


def middle(got, kept, table):
    shape = jax.ShapeDtypeStruct
    return pl.pallas_call(
        middle_kernel,
        out_shape=(shape((32, D), jnp.bfloat16), shape((8, D), jnp.bfloat16)),
        scratch_shapes=[pltpu.VMEM((8, D), jnp.float32)],
        compiler_params=pltpu.CompilerParams(vmem_limit_bytes=6 * 2**20),
        cost_estimate=pl.CostEstimate(flops=2000000, bytes_accessed=1200000, transcendentals=100),
    )(got, kept, table)


def rear_kernel(x, before, w, taps, sent, own, held, acc, g, half, sems):
    core = lax.axis_index("core")
    first = jnp.logical_and(lax.axis_index("z") == 0, lax.axis_index("y") == 0)
    step = D // 4
    copies = [
        pltpu.make_async_copy(w.at[at, 0:768], held.at[at, 0:768], sems.at[i])
        for i, at in enumerate(pl.ds(step * i, step) for i in range(4))
    ]
    copies.append(pltpu.make_async_copy(w.at[:, 768:1024], held.at[:, 768:1024], sems.at[4]))
    for copy in copies:
        copy.start()
    for i in range(4):
        copies[i].wait()
        at = slice(step * i, step * (i + 1))
        for rows, source in ((slice(0, 8), before), (slice(8, 264), x)):
            part = jnp.dot(source[:, at], held[at, :768], preferred_element_type=jnp.float32)
            acc[rows] = part if i == 0 else acc[rows] + part
    u, outer, inner = (f32(bf(acc[:, 256 * i : 256 * (i + 1)])) for i in range(3))
    row = lax.broadcasted_iota(jnp.int32, u.shape, 0)
    z = jnp.where(jnp.logical_and(first, row < 8), 0.0, inner * u)
    conv = taps[2, 1:2] * z + taps[1, 1:2] * pltpu.roll(z, 1, 0) + taps[0, 1:2] * pltpu.roll(z, 2, 0)
    g[...] = bf((outer * conv)[8:])
    for target, which in ((half, 1 - core), (own, core)):
        for i in range(4):
            target[32 * i : 32 * (i + 1)] = g[pl.ds(pl.multiple_of(64 * i + 32 * which, 16), 32)]
    copies[4].wait()
    out_product(half[...], held.at[:, 768:1024], 1.0, sent)


def rear(x, before, w, taps):
    shape = jax.ShapeDtypeStruct
    return pl.pallas_call(
        rear_kernel,
        in_specs=[VMEM, VMEM, HBM, VMEM],
        out_specs=(VMEM, VMEM),
        out_shape=(shape((128, D), jnp.bfloat16), shape((128, 256), jnp.bfloat16)),
        scratch_shapes=[
            pltpu.VMEM((D, 1024), jnp.bfloat16),
            pltpu.VMEM((264, 768), jnp.float32),
            pltpu.VMEM((256, 256), jnp.bfloat16),
            pltpu.VMEM((128, 256), jnp.bfloat16),
            pltpu.SemaphoreType.DMA((5,)),
        ],
        compiler_params=pltpu.CompilerParams(vmem_limit_bytes=50 * 2**20),
        cost_estimate=pl.CostEstimate(flops=1200000000, bytes_accessed=7000000, transcendentals=0),
    )(x, before, w, taps)


def last_kernel(got, own, table, out):
    total = f32(got[0]) + f32(got[1]) + f32(got[2]) + f32(got[3])
    alpha = (2.0 * LAYERS) ** 0.25
    state = norm(alpha * f32(own[...]) + total, table[1:2], table[3:4])
    for i in range(8):
        out[i] = state[:, 256 * i : 256 * (i + 1)]


def last(got, own, table):
    return pl.pallas_call(
        last_kernel,
        out_shape=jax.ShapeDtypeStruct((8, 32, 256), jnp.bfloat16),
        compiler_params=pltpu.CompilerParams(vmem_limit_bytes=6 * 2**20),
        cost_estimate=pl.CostEstimate(flops=2000000, bytes_accessed=1200000, transcendentals=100),
    )(got, own, table)


def solution(mesh):
    mesh = Mesh(mesh.devices.reshape(8, 8, 4, 2), ("z", "y", "x", "core"))
    in_specs = (
        P(SP, TP),
        P(None, SP, TP),
        P(None, SP, TP),
        P(None, SP, TP),
        P(None, None, TP),
        P(None, TP, SP),
        P(None, TP),
        P(None, TP),
    )
    return jax.shard_map(shards, mesh=mesh, in_specs=in_specs, out_specs=P(SP, TP), check_vma=False)
```

```python
import jax
import jax.numpy as jnp
from jax import lax
from jax.experimental import pallas as pl
from jax.experimental.pallas import tpu as pltpu
from jax.sharding import Mesh, PartitionSpec as P


D = 2048
LAYERS = 2
TP = ("x", "core")
SP = ("z", "y")
HALO = 16
IN_UP, OUT_UP = 2.0**18, 2.0**14


def bf(x):
    return x.astype(jnp.bfloat16)


def f32(x):
    return x.astype(jnp.float32)


HBM = pl.BlockSpec(memory_space=pltpu.HBM)
VMEM = pl.BlockSpec(memory_space=pltpu.VMEM)


def pack_kernel(value, outer, inner, out_t, tokens, gain, bias, early, late, copies, held, rows, left, sems):
    fills = [pltpu.make_async_copy(w, held.at[i], sems.at[i]) for i, w in enumerate((value, outer, inner, out_t))]
    fills.append(pltpu.make_async_copy(gain, left.at[0:2], sems.at[4]))
    fills.append(pltpu.make_async_copy(bias, left.at[2:4], sems.at[5]))
    fills.append(pltpu.make_async_copy(tokens, rows.at[0:256], sems.at[6]))
    for copy in fills[4:] + fills[:4]:
        copy.start()
    fills[4].wait()
    fills[5].wait()
    rest = left[...]
    terms = []
    for _ in range(3):
        terms.append(f32(bf(rest)))
        rest = rest - terms[-1]
    terms.append(jnp.zeros_like(rest))
    rows[256:] = bf(jnp.concatenate(terms, axis=0))
    fills[6].wait()
    sends = [pltpu.make_async_copy(rows, copies.at[i, HALO : HALO + 272], sems.at[7 + i]) for i in range(8)]
    for copy in sends:
        copy.start()
    for i in range(4):
        at = slice(256 * i, 256 * (i + 1))
        fills[i].wait()
        early[:, at] = bf(f32(held[i, 0]) * (IN_UP if i < 3 else OUT_UP))
        late[:, at] = held[i, 1]
    for copy in sends:
        copy.wait()


HBM = pl.BlockSpec(memory_space=pltpu.HBM)
VMEM = pl.BlockSpec(memory_space=pltpu.VMEM)


def pack(value, outer, inner, out_t, tokens, gain, bias):
    shape = jax.ShapeDtypeStruct((32, 1024), jnp.bfloat16)
    return pl.pallas_call(
        pack_kernel,
        in_specs=[HBM] * 7,
        out_specs=(VMEM, VMEM, HBM),
        out_shape=(shape, shape, jax.ShapeDtypeStruct((8, 288, 256), jnp.bfloat16)),
        scratch_shapes=[
            pltpu.VMEM((4, 2, 32, 256), jnp.bfloat16),
            pltpu.VMEM((272, 256), jnp.bfloat16),
            pltpu.VMEM((4, 256), jnp.float32),
            pltpu.SemaphoreType.DMA((15,)),
        ],
        cost_estimate=pl.CostEstimate(flops=2000000, bytes_accessed=1700000, transcendentals=0),
    )(value, outer, inner, out_t, tokens, gain, bias)


def norm(pre, gain, bias):
    mean = jnp.mean(pre, axis=-1, keepdims=True)
    cent = pre - mean
    var = jnp.mean(cent * cent, axis=-1, keepdims=True)
    return bf(cent * lax.rsqrt(var + 1e-05) * gain + bias)


def shards(tokens, value, outer, inner, taps, out, gain, bias):
    taps = jnp.swapaxes(taps, 0, 1)
    halo = lax.ppermute(tokens[-HALO:], SP, [(i, i + 1) for i in range(63)])
    early, late, copies = pack(value, outer, inner, jnp.swapaxes(out, 1, 2), tokens, gain, bias)
    late = lax.all_gather(late, SP, axis=0, tiled=True)
    copies = lax.dynamic_update_slice(copies, jnp.broadcast_to(halo[None], (8, HALO, 256)), (0, 0, 0))
    everyone = lax.all_to_all(copies, TP, 0, 0, tiled=True)
    early = lax.all_gather(early.astype(jnp.float16), SP, axis=0, tiled=True)

    weights = [bf(early[:, 256 * i : 256 * (i + 1)]) for i in range(4)]
    sent, half = front(everyone, weights, taps)
    got = lax.ppermute(sent, "core", [(0, 1), (1, 0)])
    mine, kept, table = aside(half, weights[3], everyone)
    got = lax.all_to_all(folded(got, mine), "x", 0, 0, tiled=True)
    own, before = middle(got, kept, table)
    every = lax.all_gather(own.astype(jnp.float16), TP, axis=0, tiled=True)

    sent, gated, resid = rear(bf(every), before, late, taps)
    got = lax.ppermute(sent, "core", [(0, 1), (1, 0)])
    mine = own_product(gated, late)
    got = lax.all_to_all(bf(f32(got) + f32(mine)), "x", 0, 0, tiled=True)
    pre, stats = moments(got, resid)
    return last(lax.all_to_all(stats, TP, 0, 0, tiled=True), pre, gain, bias)


def out_product(rows, w_out, down, target):
    for n in range(4):
        at = slice(512 * n, 512 * (n + 1))
        part = lax.dot_general(rows, w_out[at], (((1,), (1,)), ((), ())), preferred_element_type=jnp.float32)
        target[:, at] = bf(part * down)


def front_kernel(xs, w_u, w_outer, w_inner, w_out, taps, sent, own, x, g, half, held, sems):
    core = lax.axis_index("core")
    first = jnp.logical_and(lax.axis_index("z") == 0, lax.axis_index("y") == 0)
    rows = HALO + 256
    blocks = [
        pltpu.make_async_copy(xs.at[j, 0:rows], x.at[:, 256 * j : 256 * (j + 1)], sems.at[j]) for j in range(8)
    ]
    weight = pltpu.make_async_copy(w_out, held, sems.at[8])
    for copy in blocks:
        copy.start()
    sums = [0.0, 0.0, 0.0]
    for part in range(2):
        for copy in blocks[4 * part : 4 * (part + 1)]:
            copy.wait()
        if part == 1:
            weight.start()
        at = slice(1024 * part, 1024 * (part + 1))
        for i, w in enumerate((w_u, w_outer, w_inner)):
            sums[i] = sums[i] + jnp.dot(x[:, at], w[at], preferred_element_type=jnp.float32)
    u, outer, inner = (f32(bf(total * (1.0 / IN_UP))) for total in sums)
    row = lax.broadcasted_iota(jnp.int32, u.shape, 0)
    z = jnp.where(jnp.logical_and(first, row < HALO), 0.0, inner * u)
    conv = taps[2, 0:1] * z + taps[1, 0:1] * pltpu.roll(z, 1, 0) + taps[0, 0:1] * pltpu.roll(z, 2, 0)
    g[...] = bf(outer * conv)
    for target, which in ((half, 1 - core), (own, core)):
        target[128:] = g[HALO - 8 : HALO]
        for i in range(4):
            target[32 * i : 32 * (i + 1)] = g[pl.ds(pl.multiple_of(HALO + 64 * i + 32 * which, 16), 32)]
    weight.wait()
    out_product(half[...], held, 1.0 / OUT_UP, sent)


def front(xs, weights, taps):
    shape = jax.ShapeDtypeStruct
    return pl.pallas_call(
        front_kernel,
        in_specs=[HBM, VMEM, VMEM, VMEM, HBM, VMEM],
        out_specs=(VMEM,) * 2,
        out_shape=(shape((136, D), jnp.bfloat16), shape((136, 256), jnp.bfloat16)),
        scratch_shapes=[
            pltpu.VMEM((HALO + 256, D), jnp.bfloat16),
            pltpu.VMEM((HALO + 256, 256), jnp.bfloat16),
            pltpu.VMEM((136, 256), jnp.bfloat16),
            pltpu.VMEM((D, 256), jnp.bfloat16),
            pltpu.SemaphoreType.DMA((9,)),
        ],
        compiler_params=pltpu.CompilerParams(vmem_limit_bytes=50 * 2**20),
        cost_estimate=pl.CostEstimate(flops=1200000000, bytes_accessed=7000000, transcendentals=0),
    )(xs, *weights, taps)


def aside_kernel(rows, w, xs, mine, kept, table, held, x, tails, sems):
    tp = 2 * lax.axis_index("x") + lax.axis_index("core")
    weight = pltpu.make_async_copy(w, held, sems.at[0])
    weight.start()
    copies = []
    for j in range(8):
        at = slice(256 * j, 256 * (j + 1))
        start = pl.multiple_of(HALO + 32 * tp, 16)
        copies.append(pltpu.make_async_copy(xs.at[j, pl.ds(start, 32)], x.at[0:32, at], sems.at[1 + j]))
        copies.append(pltpu.make_async_copy(xs.at[j, HALO - 8 : HALO], x.at[32:40, at], sems.at[9 + j]))
        copies.append(pltpu.make_async_copy(xs.at[j, HALO + 256 : HALO + 272], tails.at[:, at], sems.at[17 + j]))
    for copy in copies:
        copy.start()
    weight.wait()
    out_product(rows[...], held, 1.0 / OUT_UP, mine)
    for copy in copies:
        copy.wait()
    kept[...] = (2.0 * LAYERS) ** 0.25 * f32(x[...])
    tail = f32(tails[...])
    table[...] = tail[0:4] + tail[4:8] + tail[8:12]


def aside(rows, w, xs):
    shape = jax.ShapeDtypeStruct
    return pl.pallas_call(
        aside_kernel,
        in_specs=[VMEM, HBM, HBM],
        out_specs=(VMEM,) * 3,
        out_shape=(shape((136, D), jnp.bfloat16), shape((40, D), jnp.float32), shape((4, D), jnp.float32)),
        scratch_shapes=[
            pltpu.VMEM((D, 256), jnp.bfloat16),
            pltpu.VMEM((40, D), jnp.bfloat16),
            pltpu.VMEM((16, D), jnp.bfloat16),
            pltpu.SemaphoreType.DMA((25,)),
        ],
        compiler_params=pltpu.CompilerParams(vmem_limit_bytes=52 * 2**20),
        cost_estimate=pl.CostEstimate(flops=800000000, bytes_accessed=2000000, transcendentals=0),
    )(rows, w, xs)


def fold_kernel(got, mine, out, strip):
    total = f32(got[...]) + f32(mine[...])
    for i in range(4):
        out[i, :, :D] = bf(total[32 * i : 32 * (i + 1)])
    for t in range(2):
        for r in range(16):
            strip[16 * t + r : 16 * t + r + 1] = total[134 + t : 135 + t, 128 * r : 128 * (r + 1)]
    for i in range(4):
        out[i, :, D:] = bf(strip[...])


def folded(got, mine):
    return pl.pallas_call(
        fold_kernel,
        out_shape=jax.ShapeDtypeStruct((4, 32, D + 128), jnp.bfloat16),
        scratch_shapes=[pltpu.VMEM((32, 128), jnp.float32)],
        compiler_params=pltpu.CompilerParams(vmem_limit_bytes=6 * 2**20),
        cost_estimate=pl.CostEstimate(flops=1000000, bytes_accessed=2200000, transcendentals=0),
    )(got, mine)


def middle_kernel(got, kept, table, own, before, wide):
    total = f32(got[0]) + f32(got[1]) + f32(got[2]) + f32(got[3])
    wide[...] = jnp.zeros_like(wide)
    for t in range(2):
        for r in range(16):
            wide[6 + t : 7 + t, 128 * r : 128 * (r + 1)] = total[16 * t + r : 16 * t + r + 1, D:]
    gain, bias = table[0:1], table[2:3]
    own[...] = norm(kept[:32] + total[:, :D], gain, bias)
    before[...] = norm(kept[32:] + wide[...], gain, bias)


def middle(got, kept, table):
    shape = jax.ShapeDtypeStruct
    return pl.pallas_call(
        middle_kernel,
        out_shape=(shape((32, D), jnp.bfloat16), shape((8, D), jnp.bfloat16)),
        scratch_shapes=[pltpu.VMEM((8, D), jnp.float32)],
        compiler_params=pltpu.CompilerParams(vmem_limit_bytes=6 * 2**20),
        cost_estimate=pl.CostEstimate(flops=2000000, bytes_accessed=1200000, transcendentals=100),
    )(got, kept, table)


def rear_kernel(x, before, w, taps, sent, g, resid, held, other, acc, sems):
    core = lax.axis_index("core")
    tp = 2 * lax.axis_index("x") + core
    first = jnp.logical_and(lax.axis_index("z") == 0, lax.axis_index("y") == 0)
    step = D // 4
    copies = [
        pltpu.make_async_copy(w.at[at, 0:768], held.at[at], sems.at[i])
        for i, at in enumerate(pl.ds(step * i, step) for i in range(4))
    ]
    for i in range(4):
        start = pl.multiple_of(256 * (2 * i + 1 - core), 256)
        copies.append(pltpu.make_async_copy(w.at[pl.ds(start, 256), 768:1024], other.at[i], sems.at[4 + i]))
    for copy in copies:
        copy.start()
    alpha = (2.0 * LAYERS) ** 0.25
    resid[...] = alpha * f32(x[:, pl.ds(pl.multiple_of(256 * tp, 256), 256)])
    for i in range(4):
        copies[i].wait()
        at = slice(step * i, step * (i + 1))
        for rows, source in ((slice(0, 8), before), (slice(8, 264), x)):
            part = jnp.dot(source[:, at], held[at], preferred_element_type=jnp.float32)
            acc[rows] = part if i == 0 else acc[rows] + part
    u, outer, inner = (f32(bf(acc[:, 256 * i : 256 * (i + 1)])) for i in range(3))
    row = lax.broadcasted_iota(jnp.int32, u.shape, 0)
    z = jnp.where(jnp.logical_and(first, row < 8), 0.0, inner * u)
    conv = taps[2, 1:2] * z + taps[1, 1:2] * pltpu.roll(z, 1, 0) + taps[0, 1:2] * pltpu.roll(z, 2, 0)
    g[...] = bf((outer * conv)[8:])
    for i in range(4):
        copies[4 + i].wait()
        sent[i] = bf(times_turned(g[...], other[i]))


def times_turned(a, b):
    return lax.dot_general(a, b, (((1,), (1,)), ((), ())), preferred_element_type=jnp.float32)


def rear(x, before, w, taps):
    shape = jax.ShapeDtypeStruct
    return pl.pallas_call(
        rear_kernel,
        in_specs=[VMEM, VMEM, HBM, VMEM],
        out_specs=(VMEM,) * 3,
        out_shape=(
            shape((4, 256, 256), jnp.bfloat16),
            shape((256, 256), jnp.bfloat16),
            shape((256, 256), jnp.float32),
        ),
        scratch_shapes=[
            pltpu.VMEM((D, 768), jnp.bfloat16),
            pltpu.VMEM((4, 256, 256), jnp.bfloat16),
            pltpu.VMEM((264, 768), jnp.float32),
            pltpu.SemaphoreType.DMA((8,)),
        ],
        compiler_params=pltpu.CompilerParams(vmem_limit_bytes=50 * 2**20),
        cost_estimate=pl.CostEstimate(flops=1200000000, bytes_accessed=7000000, transcendentals=0),
    )(x, before, w, taps)


def own_kernel(g, w, mine, held, sems):
    core = lax.axis_index("core")
    copies = []
    for i in range(4):
        start = pl.multiple_of(256 * (2 * i + core), 256)
        copies.append(pltpu.make_async_copy(w.at[pl.ds(start, 256), 768:1024], held.at[i], sems.at[i]))
    for copy in copies:
        copy.start()
    for i in range(4):
        copies[i].wait()
        mine[i] = bf(times_turned(g[...], held[i]))


def own_product(g, w):
    return pl.pallas_call(
        own_kernel,
        in_specs=[VMEM, HBM],
        out_specs=VMEM,
        out_shape=jax.ShapeDtypeStruct((4, 256, 256), jnp.bfloat16),
        scratch_shapes=[pltpu.VMEM((4, 256, 256), jnp.bfloat16), pltpu.SemaphoreType.DMA((4,))],
        compiler_params=pltpu.CompilerParams(vmem_limit_bytes=52 * 2**20),
        cost_estimate=pl.CostEstimate(flops=800000000, bytes_accessed=2000000, transcendentals=0),
    )(g, w)


def moment_kernel(got, resid, pre, stats):
    total = resid[...] + f32(got[0]) + f32(got[1]) + f32(got[2]) + f32(got[3])
    pre[...] = total
    ones = jnp.ones((8, 256), jnp.float32)
    along = lambda v: lax.dot_general(
        ones, v, (((1,), (1,)), ((), ())), precision=lax.Precision.HIGHEST, preferred_element_type=jnp.float32
    )
    cent = total - jnp.mean(total, axis=-1, keepdims=True)
    row = lax.broadcasted_iota(jnp.int32, (8, 256), 0)
    both = jnp.where(row == 0, along(total) * (1.0 / 256), along(cent * cent))
    for i in range(8):
        stats[i] = both


def moments(got, resid):
    shape = jax.ShapeDtypeStruct
    return pl.pallas_call(
        moment_kernel,
        out_shape=(shape((256, 256), jnp.float32), shape((8, 8, 256), jnp.float32)),
        compiler_params=pltpu.CompilerParams(vmem_limit_bytes=6 * 2**20),
        cost_estimate=pl.CostEstimate(flops=2000000, bytes_accessed=1200000, transcendentals=100),
    )(got, resid)


def last_kernel(stats, pre, gain, bias, out):
    means = jnp.concatenate([stats[i, 0:1] for i in range(8)], axis=0)
    spread = jnp.concatenate([stats[i, 1:2] for i in range(8)], axis=0)
    mean = jnp.mean(means, axis=0, keepdims=True)
    off = means - mean
    var = (jnp.sum(spread, axis=0, keepdims=True) + 256.0 * jnp.sum(off * off, axis=0, keepdims=True)) * (1.0 / D)
    turned = lambda v: jnp.concatenate([jnp.transpose(jnp.broadcast_to(v, (128, 256)))] * 2, axis=1)
    state = (pre[...] - turned(mean)) * turned(lax.rsqrt(var + 1e-05))
    out[...] = bf(state * gain[1:2] + bias[1:2])


def last(stats, pre, gain, bias):
    return pl.pallas_call(
        last_kernel,
        out_shape=jax.ShapeDtypeStruct((256, 256), jnp.bfloat16),
        compiler_params=pltpu.CompilerParams(vmem_limit_bytes=6 * 2**20),
        cost_estimate=pl.CostEstimate(flops=2000000, bytes_accessed=1200000, transcendentals=100),
    )(stats, pre, gain, bias)


def solution(mesh):
    mesh = Mesh(mesh.devices.reshape(8, 8, 4, 2), ("z", "y", "x", "core"))
    in_specs = (
        P(SP, TP),
        P(None, SP, TP),
        P(None, SP, TP),
        P(None, SP, TP),
        P(None, None, TP),
        P(None, TP, SP),
        P(None, TP),
        P(None, TP),
    )
    return jax.shard_map(shards, mesh=mesh, in_specs=in_specs, out_specs=P(SP, TP), check_vma=False)
```

```python
import functools

import jax
import jax.numpy as jnp
from jax import lax
from jax.experimental import pallas as pl
from jax.experimental.pallas import tpu as pltpu
from jax.sharding import Mesh, PartitionSpec as P


D = 2048
LAYERS = 2
TP = ("x", "core")
SP = ("z", "y")
HALO = 16
IN_UP, OUT_UP = 2.0**18, 2.0**14


def bf(x):
    return x.astype(jnp.bfloat16)


def f32(x):
    return x.astype(jnp.float32)


HBM = pl.BlockSpec(memory_space=pltpu.HBM)
VMEM = pl.BlockSpec(memory_space=pltpu.VMEM)


def pack_kernel(value, outer, inner, out_t, tokens, gain, bias, early, late, copies, held, rows, left, sems):
    fills = [pltpu.make_async_copy(w, held.at[i], sems.at[i]) for i, w in enumerate((value, outer, inner, out_t))]
    fills.append(pltpu.make_async_copy(gain, left.at[0:2], sems.at[4]))
    fills.append(pltpu.make_async_copy(bias, left.at[2:4], sems.at[5]))
    fills.append(pltpu.make_async_copy(tokens, rows.at[0:256], sems.at[6]))
    for copy in fills[4:] + fills[:4]:
        copy.start()
    fills[4].wait()
    fills[5].wait()
    rest = left[...]
    terms = []
    for _ in range(3):
        terms.append(f32(bf(rest)))
        rest = rest - terms[-1]
    terms.append(jnp.zeros_like(rest))
    rows[256:] = bf(jnp.concatenate(terms, axis=0))
    fills[6].wait()
    sends = [pltpu.make_async_copy(rows, copies.at[i, HALO : HALO + 272], sems.at[7 + i]) for i in range(8)]
    for copy in sends:
        copy.start()
    for i in range(4):
        at = slice(256 * i, 256 * (i + 1))
        fills[i].wait()
        early[:, at] = bf(f32(held[i, 0]) * (IN_UP if i < 3 else OUT_UP))
        late[:, at] = held[i, 1]
    for copy in sends:
        copy.wait()


HBM = pl.BlockSpec(memory_space=pltpu.HBM)
VMEM = pl.BlockSpec(memory_space=pltpu.VMEM)


def pack(value, outer, inner, out_t, tokens, gain, bias):
    shape = jax.ShapeDtypeStruct((32, 1024), jnp.bfloat16)
    return pl.pallas_call(
        pack_kernel,
        in_specs=[HBM] * 7,
        out_specs=(VMEM, VMEM, HBM),
        out_shape=(shape, shape, jax.ShapeDtypeStruct((8, 288, 256), jnp.bfloat16)),
        scratch_shapes=[
            pltpu.VMEM((4, 2, 32, 256), jnp.bfloat16),
            pltpu.VMEM((272, 256), jnp.bfloat16),
            pltpu.VMEM((4, 256), jnp.float32),
            pltpu.SemaphoreType.DMA((15,)),
        ],
        cost_estimate=pl.CostEstimate(flops=2000000, bytes_accessed=1700000, transcendentals=0),
    )(value, outer, inner, out_t, tokens, gain, bias)


def norm(pre, gain, bias):
    mean = jnp.mean(pre, axis=-1, keepdims=True)
    cent = pre - mean
    var = jnp.mean(cent * cent, axis=-1, keepdims=True)
    return bf(cent * lax.rsqrt(var + 1e-05) * gain + bias)


def shards(tokens, value, outer, inner, taps, out, gain, bias):
    taps = jnp.swapaxes(taps, 0, 1)
    halo = lax.ppermute(tokens[-HALO:], SP, [(i, i + 1) for i in range(63)])
    early, late, copies = pack(value, outer, inner, jnp.swapaxes(out, 1, 2), tokens, gain, bias)
    late = lax.all_gather(late, SP, axis=0, tiled=True)
    copies = lax.dynamic_update_slice(copies, jnp.broadcast_to(halo[None], (8, HALO, 256)), (0, 0, 0))
    everyone = lax.all_to_all(copies, TP, 0, 0, tiled=True)
    early = lax.all_gather(early.astype(jnp.float16), SP, axis=0, tiled=True)

    weights = [bf(early[:, 256 * i : 256 * (i + 1)]) for i in range(4)]
    sent, half = front(everyone, weights, taps)
    got = lax.ppermute(sent, "core", [(0, 1), (1, 0)])
    mine, kept, table = aside(half, weights[3], everyone)
    got = lax.all_to_all(folded(got, mine), "x", 0, 0, tiled=True)
    own, before = middle(got, kept, table)
    every = lax.all_gather(own.astype(jnp.float16), TP, axis=0, tiled=True)

    sent, half = rear(bf(every), before, late, taps)
    got = lax.ppermute(sent, "core", [(0, 1), (1, 0)])
    mine = own_product(half, late, 768, 1.0, 52)
    got = lax.all_to_all(bf(f32(got) + f32(mine)).reshape(4, 32, D), "x", 0, 0, tiled=True)
    return lax.all_to_all(last(got, own, table), TP, 0, 0, tiled=True).reshape(256, 256)


def out_product(rows, w_out, down, target):
    for n in range(4):
        at = slice(512 * n, 512 * (n + 1))
        part = lax.dot_general(rows, w_out[at], (((1,), (1,)), ((), ())), preferred_element_type=jnp.float32)
        target[:, at] = bf(part * down)


def front_kernel(xs, w_u, w_outer, w_inner, w_out, taps, sent, own, x, g, half, held, parts, sems):
    core = lax.axis_index("core")
    first = jnp.logical_and(lax.axis_index("z") == 0, lax.axis_index("y") == 0)
    rows = HALO + 256
    blocks = [
        pltpu.make_async_copy(xs.at[4 * i : 4 * (i + 1), 0:rows], parts.at[4 * i : 4 * (i + 1)], sems.at[i])
        for i in range(2)
    ]
    weight = pltpu.make_async_copy(w_out, held, sems.at[2])
    for copy in blocks:
        copy.start()
    sums = [0.0, 0.0, 0.0]
    for part in range(2):
        blocks[part].wait()
        if part == 1:
            weight.start()
        for j in range(4 * part, 4 * (part + 1)):
            x[:, 256 * j : 256 * (j + 1)] = parts[j]
        at = slice(1024 * part, 1024 * (part + 1))
        for i, w in enumerate((w_u, w_outer, w_inner)):
            sums[i] = sums[i] + jnp.dot(x[:, at], w[at], preferred_element_type=jnp.float32)
    u, outer, inner = (f32(bf(total * (1.0 / IN_UP))) for total in sums)
    row = lax.broadcasted_iota(jnp.int32, u.shape, 0)
    z = jnp.where(jnp.logical_and(first, row < HALO), 0.0, inner * u)
    conv = taps[2, 0:1] * z + taps[1, 0:1] * pltpu.roll(z, 1, 0) + taps[0, 0:1] * pltpu.roll(z, 2, 0)
    g[...] = bf(outer * conv)
    for target, which in ((half, 1 - core), (own, core)):
        target[128:] = g[HALO - 8 : HALO]
        for i in range(4):
            target[32 * i : 32 * (i + 1)] = g[pl.ds(pl.multiple_of(HALO + 64 * i + 32 * which, 16), 32)]
    weight.wait()
    out_product(half[...], held, 1.0 / OUT_UP, sent)


def front(xs, weights, taps):
    shape = jax.ShapeDtypeStruct
    return pl.pallas_call(
        front_kernel,
        in_specs=[HBM, VMEM, VMEM, VMEM, HBM, VMEM],
        out_specs=(VMEM,) * 2,
        out_shape=(shape((136, D), jnp.bfloat16), shape((136, 256), jnp.bfloat16)),
        scratch_shapes=[
            pltpu.VMEM((HALO + 256, D), jnp.bfloat16),
            pltpu.VMEM((HALO + 256, 256), jnp.bfloat16),
            pltpu.VMEM((136, 256), jnp.bfloat16),
            pltpu.VMEM((D, 256), jnp.bfloat16),
            pltpu.VMEM((8, HALO + 256, 256), jnp.bfloat16),
            pltpu.SemaphoreType.DMA((3,)),
        ],
        compiler_params=pltpu.CompilerParams(vmem_limit_bytes=50 * 2**20),
        cost_estimate=pl.CostEstimate(flops=1200000000, bytes_accessed=7000000, transcendentals=0),
    )(xs, *weights, taps)


def aside_kernel(rows, w, xs, mine, kept, table, held, x, tails, sems):
    tp = 2 * lax.axis_index("x") + lax.axis_index("core")
    weight = pltpu.make_async_copy(w, held, sems.at[0])
    weight.start()
    start = pl.multiple_of(HALO + 32 * tp, 16)
    copies = [
        pltpu.make_async_copy(xs.at[:, pl.ds(start, 32)], x.at[:, 0:32], sems.at[1]),
        pltpu.make_async_copy(xs.at[:, HALO - 8 : HALO], x.at[:, 32:40], sems.at[2]),
        pltpu.make_async_copy(xs.at[:, HALO + 256 : HALO + 272], tails, sems.at[3]),
    ]
    for copy in copies:
        copy.start()
    weight.wait()
    out_product(rows[...], held, 1.0 / OUT_UP, mine)
    for copy in copies:
        copy.wait()
    for j in range(8):
        at = slice(256 * j, 256 * (j + 1))
        kept[:, at] = (2.0 * LAYERS) ** 0.25 * f32(x[j])
        tail = f32(tails[j])
        table[:, at] = tail[0:4] + tail[4:8] + tail[8:12]


def aside(rows, w, xs):
    shape = jax.ShapeDtypeStruct
    return pl.pallas_call(
        aside_kernel,
        in_specs=[VMEM, HBM, HBM],
        out_specs=(VMEM,) * 3,
        out_shape=(shape((136, D), jnp.bfloat16), shape((40, D), jnp.float32), shape((4, D), jnp.float32)),
        scratch_shapes=[
            pltpu.VMEM((D, 256), jnp.bfloat16),
            pltpu.VMEM((8, 40, 256), jnp.bfloat16),
            pltpu.VMEM((8, 16, 256), jnp.bfloat16),
            pltpu.SemaphoreType.DMA((4,)),
        ],
        compiler_params=pltpu.CompilerParams(vmem_limit_bytes=52 * 2**20),
        cost_estimate=pl.CostEstimate(flops=800000000, bytes_accessed=2000000, transcendentals=0),
    )(rows, w, xs)


def own_kernel(column, down, rows, w, mine, held, sems):
    copies = [
        pltpu.make_async_copy(w.at[at, column : column + 256], held.at[at], sems.at[i])
        for i, at in enumerate(pl.ds(512 * i, 512) for i in range(4))
    ]
    for copy in copies:
        copy.start()
    for i in range(4):
        copies[i].wait()
        at = slice(512 * i, 512 * (i + 1))
        part = lax.dot_general(rows[...], held[at], (((1,), (1,)), ((), ())), preferred_element_type=jnp.float32)
        mine[:, at] = bf(part * down)


def own_product(rows, w, column, down, limit):
    return pl.pallas_call(
        functools.partial(own_kernel, column, down),
        in_specs=[VMEM, HBM],
        out_specs=VMEM,
        out_shape=jax.ShapeDtypeStruct((rows.shape[0], D), jnp.bfloat16),
        scratch_shapes=[pltpu.VMEM((D, 256), jnp.bfloat16), pltpu.SemaphoreType.DMA((4,))],
        compiler_params=pltpu.CompilerParams(vmem_limit_bytes=limit * 2**20),
        cost_estimate=pl.CostEstimate(flops=800000000, bytes_accessed=2000000, transcendentals=0),
    )(rows, w)


def fold_kernel(got, mine, out, strip):
    total = f32(got[...]) + f32(mine[...])
    for i in range(4):
        out[i, :, :D] = bf(total[32 * i : 32 * (i + 1)])
    for t in range(2):
        for r in range(16):
            strip[16 * t + r : 16 * t + r + 1] = total[134 + t : 135 + t, 128 * r : 128 * (r + 1)]
    for i in range(4):
        out[i, :, D:] = bf(strip[...])


def folded(got, mine):
    return pl.pallas_call(
        fold_kernel,
        out_shape=jax.ShapeDtypeStruct((4, 32, D + 128), jnp.bfloat16),
        scratch_shapes=[pltpu.VMEM((32, 128), jnp.float32)],
        compiler_params=pltpu.CompilerParams(vmem_limit_bytes=6 * 2**20),
        cost_estimate=pl.CostEstimate(flops=1000000, bytes_accessed=2200000, transcendentals=0),
    )(got, mine)


def middle_kernel(got, kept, table, own, before, wide):
    total = f32(got[0]) + f32(got[1]) + f32(got[2]) + f32(got[3])
    wide[...] = jnp.zeros_like(wide)
    for t in range(2):
        for r in range(16):
            wide[6 + t : 7 + t, 128 * r : 128 * (r + 1)] = total[16 * t + r : 16 * t + r + 1, D:]
    gain, bias = table[0:1], table[2:3]
    own[...] = norm(kept[:32] + total[:, :D], gain, bias)
    before[...] = norm(kept[32:] + wide[...], gain, bias)


def middle(got, kept, table):
    shape = jax.ShapeDtypeStruct
    return pl.pallas_call(
        middle_kernel,
        out_shape=(shape((32, D), jnp.bfloat16), shape((8, D), jnp.bfloat16)),
        scratch_shapes=[pltpu.VMEM((8, D), jnp.float32)],
        compiler_params=pltpu.CompilerParams(vmem_limit_bytes=6 * 2**20),
        cost_estimate=pl.CostEstimate(flops=2000000, bytes_accessed=1200000, transcendentals=100),
    )(got, kept, table)


def rear_kernel(x, before, w, taps, sent, own, held, acc, g, half, sems):
    core = lax.axis_index("core")
    first = jnp.logical_and(lax.axis_index("z") == 0, lax.axis_index("y") == 0)
    step = D // 4
    copies = [
        pltpu.make_async_copy(w.at[at, 0:768], held.at[at, 0:768], sems.at[i])
        for i, at in enumerate(pl.ds(step * i, step) for i in range(4))
    ]
    copies.append(pltpu.make_async_copy(w.at[:, 768:1024], held.at[:, 768:1024], sems.at[4]))
    for copy in copies:
        copy.start()
    for i in range(4):
        copies[i].wait()
        at = slice(step * i, step * (i + 1))
        for rows, source in ((slice(0, 8), before), (slice(8, 264), x)):
            part = jnp.dot(source[:, at], held[at, :768], preferred_element_type=jnp.float32)
            acc[rows] = part if i == 0 else acc[rows] + part
    u, outer, inner = (f32(bf(acc[:, 256 * i : 256 * (i + 1)])) for i in range(3))
    row = lax.broadcasted_iota(jnp.int32, u.shape, 0)
    z = jnp.where(jnp.logical_and(first, row < 8), 0.0, inner * u)
    conv = taps[2, 1:2] * z + taps[1, 1:2] * pltpu.roll(z, 1, 0) + taps[0, 1:2] * pltpu.roll(z, 2, 0)
    g[...] = bf((outer * conv)[8:])
    for target, which in ((half, 1 - core), (own, core)):
        for i in range(4):
            target[32 * i : 32 * (i + 1)] = g[pl.ds(pl.multiple_of(64 * i + 32 * which, 16), 32)]
    copies[4].wait()
    out_product(half[...], held.at[:, 768:1024], 1.0, sent)


def rear(x, before, w, taps):
    shape = jax.ShapeDtypeStruct
    return pl.pallas_call(
        rear_kernel,
        in_specs=[VMEM, VMEM, HBM, VMEM],
        out_specs=(VMEM, VMEM),
        out_shape=(shape((128, D), jnp.bfloat16), shape((128, 256), jnp.bfloat16)),
        scratch_shapes=[
            pltpu.VMEM((D, 1024), jnp.bfloat16),
            pltpu.VMEM((264, 768), jnp.float32),
            pltpu.VMEM((256, 256), jnp.bfloat16),
            pltpu.VMEM((128, 256), jnp.bfloat16),
            pltpu.SemaphoreType.DMA((5,)),
        ],
        compiler_params=pltpu.CompilerParams(vmem_limit_bytes=50 * 2**20),
        cost_estimate=pl.CostEstimate(flops=1200000000, bytes_accessed=7000000, transcendentals=0),
    )(x, before, w, taps)


def last_kernel(got, own, table, out):
    total = f32(got[0]) + f32(got[1]) + f32(got[2]) + f32(got[3])
    alpha = (2.0 * LAYERS) ** 0.25
    state = norm(alpha * f32(own[...]) + total, table[1:2], table[3:4])
    for i in range(8):
        out[i] = state[:, 256 * i : 256 * (i + 1)]


def last(got, own, table):
    return pl.pallas_call(
        last_kernel,
        out_shape=jax.ShapeDtypeStruct((8, 32, 256), jnp.bfloat16),
        compiler_params=pltpu.CompilerParams(vmem_limit_bytes=6 * 2**20),
        cost_estimate=pl.CostEstimate(flops=2000000, bytes_accessed=1200000, transcendentals=100),
    )(got, own, table)


def solution(mesh):
    mesh = Mesh(mesh.devices.reshape(8, 8, 4, 2), ("z", "y", "x", "core"))
    in_specs = (
        P(SP, TP),
        P(None, SP, TP),
        P(None, SP, TP),
        P(None, SP, TP),
        P(None, None, TP),
        P(None, TP, SP),
        P(None, TP),
        P(None, TP),
    )
    return jax.shard_map(shards, mesh=mesh, in_specs=in_specs, out_specs=P(SP, TP), check_vma=False)
```

```python
import functools

import jax
import jax.numpy as jnp
from jax import lax
from jax.experimental import pallas as pl
from jax.experimental.pallas import tpu as pltpu
from jax.sharding import Mesh, PartitionSpec as P


D = 2048
LAYERS = 2
TP = ("x", "core")
SP = ("z", "y")
HALO = 16
IN_UP, OUT_UP = 2.0**18, 2.0**14


def bf(x):
    return x.astype(jnp.bfloat16)


def f32(x):
    return x.astype(jnp.float32)


HBM = pl.BlockSpec(memory_space=pltpu.HBM)
VMEM = pl.BlockSpec(memory_space=pltpu.VMEM)


def pack_kernel(value, outer, inner, out_t, tokens, gain, bias, early, late, copies, held, rows, left, sems):
    fills = [pltpu.make_async_copy(w, held.at[i], sems.at[i]) for i, w in enumerate((value, outer, inner, out_t))]
    fills.append(pltpu.make_async_copy(gain, left.at[0:2], sems.at[4]))
    fills.append(pltpu.make_async_copy(bias, left.at[2:4], sems.at[5]))
    fills.append(pltpu.make_async_copy(tokens, rows.at[0:256], sems.at[6]))
    for copy in fills[4:] + fills[:4]:
        copy.start()
    fills[4].wait()
    fills[5].wait()
    rest = left[...]
    terms = []
    for _ in range(3):
        terms.append(f32(bf(rest)))
        rest = rest - terms[-1]
    terms.append(jnp.zeros_like(rest))
    rows[256:] = bf(jnp.concatenate(terms, axis=0))
    fills[6].wait()
    sends = [pltpu.make_async_copy(rows, copies.at[i, HALO : HALO + 272], sems.at[7 + i]) for i in range(8)]
    for copy in sends:
        copy.start()
    for i in range(4):
        at = slice(256 * i, 256 * (i + 1))
        fills[i].wait()
        early[:, at] = bf(f32(held[i, 0]) * (IN_UP if i < 3 else OUT_UP))
        late[:, at] = held[i, 1]
    for copy in sends:
        copy.wait()


HBM = pl.BlockSpec(memory_space=pltpu.HBM)
VMEM = pl.BlockSpec(memory_space=pltpu.VMEM)


def pack(value, outer, inner, out_t, tokens, gain, bias):
    shape = jax.ShapeDtypeStruct((32, 1024), jnp.bfloat16)
    return pl.pallas_call(
        pack_kernel,
        in_specs=[HBM] * 7,
        out_specs=(VMEM, VMEM, HBM),
        out_shape=(shape, shape, jax.ShapeDtypeStruct((8, 288, 256), jnp.bfloat16)),
        scratch_shapes=[
            pltpu.VMEM((4, 2, 32, 256), jnp.bfloat16),
            pltpu.VMEM((272, 256), jnp.bfloat16),
            pltpu.VMEM((4, 256), jnp.float32),
            pltpu.SemaphoreType.DMA((15,)),
        ],
        cost_estimate=pl.CostEstimate(flops=2000000, bytes_accessed=1700000, transcendentals=0),
    )(value, outer, inner, out_t, tokens, gain, bias)


def norm(pre, gain, bias):
    mean = jnp.mean(pre, axis=-1, keepdims=True)
    cent = pre - mean
    var = jnp.mean(cent * cent, axis=-1, keepdims=True)
    return bf(cent * lax.rsqrt(var + 1e-05) * gain + bias)


def shards(tokens, value, outer, inner, taps, out, gain, bias):
    taps = jnp.swapaxes(taps, 0, 1)
    halo = lax.ppermute(tokens[-HALO:], SP, [(i, i + 1) for i in range(63)])
    early, late, copies = pack(value, outer, inner, jnp.swapaxes(out, 1, 2), tokens, gain, bias)
    late = lax.all_gather(late, SP, axis=0, tiled=True)
    copies = lax.dynamic_update_slice(copies, jnp.broadcast_to(halo[None], (8, HALO, 256)), (0, 0, 0))
    everyone = lax.all_to_all(copies, TP, 0, 0, tiled=True)
    early = lax.all_gather(early.astype(jnp.float16), SP, axis=0, tiled=True)

    weights = [bf(early[:, 256 * i : 256 * (i + 1)]) for i in range(4)]
    sent, half = front(everyone, weights, taps)
    got = lax.ppermute(sent, "core", [(0, 1), (1, 0)])
    mine, kept, table = aside(half, weights[3], everyone)
    got = lax.all_to_all(folded(got, mine), "x", 0, 0, tiled=True)
    own, before = middle(got, kept, table)
    every = lax.all_gather(own.astype(jnp.float16), TP, axis=0, tiled=True)

    sent, half = rear(bf(every), before, late, taps)
    got = lax.ppermute(sent, "core", [(0, 1), (1, 0)])
    mine = own_product(half, late, 768, 1.0, 52)
    got = lax.all_to_all(bf(f32(got) + f32(mine)).reshape(4, 32, D), "x", 0, 0, tiled=True)
    return lax.all_to_all(last(got, own, table), TP, 0, 0, tiled=True).reshape(256, 256)


def out_product(rows, w_out, down, target):
    for n in range(4):
        at = slice(512 * n, 512 * (n + 1))
        part = lax.dot_general(rows, w_out[at], (((1,), (1,)), ((), ())), preferred_element_type=jnp.float32)
        target[:, at] = bf(part * down)


def front_kernel(xs, w_u, w_outer, w_inner, w_out, taps, sent, own, x, g, half, held, parts, sems):
    core = lax.axis_index("core")
    first = jnp.logical_and(lax.axis_index("z") == 0, lax.axis_index("y") == 0)
    rows = HALO + 256
    blocks = [
        pltpu.make_async_copy(xs.at[4 * i : 4 * (i + 1), 0:rows], parts.at[4 * i : 4 * (i + 1)], sems.at[i])
        for i in range(2)
    ]
    weight = pltpu.make_async_copy(w_out, held, sems.at[2])
    for copy in blocks:
        copy.start()
    sums = [0.0, 0.0, 0.0]
    for part in range(2):
        blocks[part].wait()
        if part == 0:
            weight.start()
        for j in range(4 * part, 4 * (part + 1)):
            x[:, 256 * j : 256 * (j + 1)] = parts[j]
        at = slice(1024 * part, 1024 * (part + 1))
        for i, w in enumerate((w_u, w_outer, w_inner)):
            sums[i] = sums[i] + jnp.dot(x[:, at], w[at], preferred_element_type=jnp.float32)
    u, outer, inner = (f32(bf(total * (1.0 / IN_UP))) for total in sums)
    row = lax.broadcasted_iota(jnp.int32, u.shape, 0)
    z = jnp.where(jnp.logical_and(first, row < HALO), 0.0, inner * u)
    conv = taps[2, 0:1] * z + taps[1, 0:1] * pltpu.roll(z, 1, 0) + taps[0, 0:1] * pltpu.roll(z, 2, 0)
    g[...] = bf(outer * conv)
    for target, which in ((half, 1 - core), (own, core)):
        target[128:] = g[HALO - 8 : HALO]
        for i in range(4):
            target[32 * i : 32 * (i + 1)] = g[pl.ds(pl.multiple_of(HALO + 64 * i + 32 * which, 16), 32)]
    weight.wait()
    out_product(half[...], held, 1.0 / OUT_UP, sent)


def front(xs, weights, taps):
    shape = jax.ShapeDtypeStruct
    return pl.pallas_call(
        front_kernel,
        in_specs=[HBM, VMEM, VMEM, VMEM, HBM, VMEM],
        out_specs=(VMEM,) * 2,
        out_shape=(shape((136, D), jnp.bfloat16), shape((136, 256), jnp.bfloat16)),
        scratch_shapes=[
            pltpu.VMEM((HALO + 256, D), jnp.bfloat16),
            pltpu.VMEM((HALO + 256, 256), jnp.bfloat16),
            pltpu.VMEM((136, 256), jnp.bfloat16),
            pltpu.VMEM((D, 256), jnp.bfloat16),
            pltpu.VMEM((8, HALO + 256, 256), jnp.bfloat16),
            pltpu.SemaphoreType.DMA((3,)),
        ],
        compiler_params=pltpu.CompilerParams(vmem_limit_bytes=50 * 2**20),
        cost_estimate=pl.CostEstimate(flops=1200000000, bytes_accessed=7000000, transcendentals=0),
    )(xs, *weights, taps)


def aside_kernel(rows, w, xs, mine, kept, table, held, x, tails, sems):
    tp = 2 * lax.axis_index("x") + lax.axis_index("core")
    weight = pltpu.make_async_copy(w, held, sems.at[0])
    weight.start()
    start = pl.multiple_of(HALO + 32 * tp, 16)
    copies = [
        pltpu.make_async_copy(xs.at[:, pl.ds(start, 32)], x.at[:, 0:32], sems.at[1]),
        pltpu.make_async_copy(xs.at[:, HALO - 8 : HALO], x.at[:, 32:40], sems.at[2]),
        pltpu.make_async_copy(xs.at[:, HALO + 256 : HALO + 272], tails, sems.at[3]),
    ]
    for copy in copies:
        copy.start()
    weight.wait()
    out_product(rows[...], held, 1.0 / OUT_UP, mine)
    for copy in copies:
        copy.wait()
    for j in range(8):
        at = slice(256 * j, 256 * (j + 1))
        kept[:, at] = (2.0 * LAYERS) ** 0.25 * f32(x[j])
        tail = f32(tails[j])
        table[:, at] = tail[0:4] + tail[4:8] + tail[8:12]


def aside(rows, w, xs):
    shape = jax.ShapeDtypeStruct
    return pl.pallas_call(
        aside_kernel,
        in_specs=[VMEM, HBM, HBM],
        out_specs=(VMEM,) * 3,
        out_shape=(shape((136, D), jnp.bfloat16), shape((40, D), jnp.float32), shape((4, D), jnp.float32)),
        scratch_shapes=[
            pltpu.VMEM((D, 256), jnp.bfloat16),
            pltpu.VMEM((8, 40, 256), jnp.bfloat16),
            pltpu.VMEM((8, 16, 256), jnp.bfloat16),
            pltpu.SemaphoreType.DMA((4,)),
        ],
        compiler_params=pltpu.CompilerParams(vmem_limit_bytes=52 * 2**20),
        cost_estimate=pl.CostEstimate(flops=800000000, bytes_accessed=2000000, transcendentals=0),
    )(rows, w, xs)


def own_kernel(column, down, rows, w, mine, held, sem):
    copy = pltpu.make_async_copy(w.at[:, column : column + 256], held, sem.at[0])
    copy.start()
    copy.wait()
    out_product(rows[...], held, down, mine)


def own_product(rows, w, column, down, limit):
    return pl.pallas_call(
        functools.partial(own_kernel, column, down),
        in_specs=[VMEM, HBM],
        out_specs=VMEM,
        out_shape=jax.ShapeDtypeStruct((rows.shape[0], D), jnp.bfloat16),
        scratch_shapes=[pltpu.VMEM((D, 256), jnp.bfloat16), pltpu.SemaphoreType.DMA((1,))],
        compiler_params=pltpu.CompilerParams(vmem_limit_bytes=limit * 2**20),
        cost_estimate=pl.CostEstimate(flops=800000000, bytes_accessed=2000000, transcendentals=0),
    )(rows, w)


def fold_kernel(got, mine, out, strip):
    total = f32(got[...]) + f32(mine[...])
    for i in range(4):
        out[i, :, :D] = bf(total[32 * i : 32 * (i + 1)])
    for t in range(2):
        for r in range(16):
            strip[16 * t + r : 16 * t + r + 1] = total[134 + t : 135 + t, 128 * r : 128 * (r + 1)]
    for i in range(4):
        out[i, :, D:] = bf(strip[...])


def folded(got, mine):
    return pl.pallas_call(
        fold_kernel,
        out_shape=jax.ShapeDtypeStruct((4, 32, D + 128), jnp.bfloat16),
        scratch_shapes=[pltpu.VMEM((32, 128), jnp.float32)],
        compiler_params=pltpu.CompilerParams(vmem_limit_bytes=6 * 2**20),
        cost_estimate=pl.CostEstimate(flops=1000000, bytes_accessed=2200000, transcendentals=0),
    )(got, mine)


def middle_kernel(got, kept, table, own, before, wide):
    total = f32(got[0]) + f32(got[1]) + f32(got[2]) + f32(got[3])
    wide[...] = jnp.zeros_like(wide)
    for t in range(2):
        for r in range(16):
            wide[6 + t : 7 + t, 128 * r : 128 * (r + 1)] = total[16 * t + r : 16 * t + r + 1, D:]
    gain, bias = table[0:1], table[2:3]
    own[...] = norm(kept[:32] + total[:, :D], gain, bias)
    before[...] = norm(kept[32:] + wide[...], gain, bias)


def middle(got, kept, table):
    shape = jax.ShapeDtypeStruct
    return pl.pallas_call(
        middle_kernel,
        out_shape=(shape((32, D), jnp.bfloat16), shape((8, D), jnp.bfloat16)),
        scratch_shapes=[pltpu.VMEM((8, D), jnp.float32)],
        compiler_params=pltpu.CompilerParams(vmem_limit_bytes=6 * 2**20),
        cost_estimate=pl.CostEstimate(flops=2000000, bytes_accessed=1200000, transcendentals=100),
    )(got, kept, table)


def rear_kernel(x, before, w, taps, sent, own, held, acc, g, half, sems):
    core = lax.axis_index("core")
    first = jnp.logical_and(lax.axis_index("z") == 0, lax.axis_index("y") == 0)
    step = D // 4
    copies = [
        pltpu.make_async_copy(w.at[at, 0:768], held.at[at, 0:768], sems.at[i])
        for i, at in enumerate(pl.ds(step * i, step) for i in range(4))
    ]
    copies.append(pltpu.make_async_copy(w.at[:, 768:1024], held.at[:, 768:1024], sems.at[4]))
    for copy in copies:
        copy.start()
    for i in range(4):
        copies[i].wait()
        at = slice(step * i, step * (i + 1))
        for rows, source in ((slice(0, 8), before), (slice(8, 264), x)):
            part = jnp.dot(source[:, at], held[at, :768], preferred_element_type=jnp.float32)
            acc[rows] = part if i == 0 else acc[rows] + part
    u, outer, inner = (f32(bf(acc[:, 256 * i : 256 * (i + 1)])) for i in range(3))
    row = lax.broadcasted_iota(jnp.int32, u.shape, 0)
    z = jnp.where(jnp.logical_and(first, row < 8), 0.0, inner * u)
    conv = taps[2, 1:2] * z + taps[1, 1:2] * pltpu.roll(z, 1, 0) + taps[0, 1:2] * pltpu.roll(z, 2, 0)
    g[...] = bf((outer * conv)[8:])
    for target, which in ((half, 1 - core), (own, core)):
        for i in range(4):
            target[32 * i : 32 * (i + 1)] = g[pl.ds(pl.multiple_of(64 * i + 32 * which, 16), 32)]
    copies[4].wait()
    out_product(half[...], held.at[:, 768:1024], 1.0, sent)


def rear(x, before, w, taps):
    shape = jax.ShapeDtypeStruct
    return pl.pallas_call(
        rear_kernel,
        in_specs=[VMEM, VMEM, HBM, VMEM],
        out_specs=(VMEM, VMEM),
        out_shape=(shape((128, D), jnp.bfloat16), shape((128, 256), jnp.bfloat16)),
        scratch_shapes=[
            pltpu.VMEM((D, 1024), jnp.bfloat16),
            pltpu.VMEM((264, 768), jnp.float32),
            pltpu.VMEM((256, 256), jnp.bfloat16),
            pltpu.VMEM((128, 256), jnp.bfloat16),
            pltpu.SemaphoreType.DMA((5,)),
        ],
        compiler_params=pltpu.CompilerParams(vmem_limit_bytes=50 * 2**20),
        cost_estimate=pl.CostEstimate(flops=1200000000, bytes_accessed=7000000, transcendentals=0),
    )(x, before, w, taps)


def last_kernel(got, own, table, out):
    total = f32(got[0]) + f32(got[1]) + f32(got[2]) + f32(got[3])
    alpha = (2.0 * LAYERS) ** 0.25
    state = norm(alpha * f32(own[...]) + total, table[1:2], table[3:4])
    for i in range(8):
        out[i] = state[:, 256 * i : 256 * (i + 1)]


def last(got, own, table):
    return pl.pallas_call(
        last_kernel,
        out_shape=jax.ShapeDtypeStruct((8, 32, 256), jnp.bfloat16),
        compiler_params=pltpu.CompilerParams(vmem_limit_bytes=6 * 2**20),
        cost_estimate=pl.CostEstimate(flops=2000000, bytes_accessed=1200000, transcendentals=100),
    )(got, own, table)


def solution(mesh):
    mesh = Mesh(mesh.devices.reshape(8, 8, 4, 2), ("z", "y", "x", "core"))
    in_specs = (
        P(SP, TP),
        P(None, SP, TP),
        P(None, SP, TP),
        P(None, SP, TP),
        P(None, None, TP),
        P(None, TP, SP),
        P(None, TP),
        P(None, TP),
    )
    return jax.shard_map(shards, mesh=mesh, in_specs=in_specs, out_specs=P(SP, TP), check_vma=False)
```
